256 devices in a mesh: grp: 2 (over y), sp: 16 (over z), tp: 4 (over x), dp: 2 (over core).
Axes of the slice: x: 4, y: 2, z: 16, core: 2. Of those that a mesh axis runs over, the one named last changes fastest.
The devices are a block of a 4x16x16 slice.
Arguments:
- latent: bfloat16 [24576, 4096], P(('grp', 'sp', 'dp')), parts along dimension 0, may hold values from -6 to 6
- context: bfloat16 [1024, 4096], P(('grp', 'sp')), parts along dimension 0, may hold values from -6 to 6
- condition: bfloat16 [8192], P('grp'), parts along dimension 0, may hold values from -6 to 6
- context_condition: bfloat16 [4096], replicated, may hold values from -6 to 6
- shift_weight: bfloat16 [4096, 4096], P('sp', ('tp', 'dp')), may hold values from -0.09375 to 0.09375
- scale_weight: bfloat16 [4096, 4096], P('sp', ('tp', 'dp')), may hold values from -0.09375 to 0.09375
- gate_weight: bfloat16 [4096, 4096], P('sp', ('tp', 'dp')), may hold values from -0.09375 to 0.09375
- norm_gain: float32 [4096], replicated, may hold values from 0.1 to 1.9
- out_gate_weight: bfloat16 [4096, 2048], P(None, ('tp', 'dp')), may hold values from -0.09375 to 0.09375
- signal_weight: bfloat16 [4096, 2048], P(None, ('tp', 'dp')), may hold values from -0.09375 to 0.09375
- writer_weight: bfloat16 [4096, 1024], P(None, ('tp', 'dp')), may hold values from -0.09375 to 0.09375
- reader_matrix: bfloat16 [4096, 1024], P(None, ('tp', 'dp')), may hold values from -0.09375 to 0.09375
- step_weight: bfloat16 [2, 4096, 32], P(None, None, ('tp', 'dp')), may hold values from -0.09375 to 0.09375
- signal_taps: float32 [3, 2048], P(None, ('tp', 'dp')), may hold values from -3.5 to 3.5
- writer_taps: float32 [3, 1024], P(None, ('tp', 'dp')), may hold values from -3.5 to 3.5
- reader_taps: float32 [3, 1024], P(None, ('tp', 'dp')), may hold values from -3.5 to 3.5
- step_bias: float32 [2, 32], P(None, ('tp', 'dp')), may hold values from -4.5 to -2.5
- decay_log: float32 [2, 32], P(None, ('tp', 'dp')), may hold values from -12 to 1
- decay_extra: float32 [2, 32, 24576], P(None, ('tp', 'dp'), ('grp', 'sp')), parts along dimension 2, may hold values from -3 to 0
- group_gain: float32 [2048], P(('tp', 'dp')), may hold values from 0.1 to 1.9
- output_weight: bfloat16 [2048, 4096], P(None, ('tp', 'dp')), may hold values from -0.125 to 0.125
Outputs:
- updated: bfloat16 [24576, 4096], P(('grp', 'sp'), ('tp', 'dp')), parts along dimension 0
The draws below stay inside these ranges and needn't reach their ends.
There are 2 independent parts, one for each index of `grp`. The reference program is written for one: setup_inputs(seed, part) draws one part's arguments, and reference() takes and returns one part's arrays. A program takes and returns all parts, laid end to end along the dimension named above; an argument that names none is the same for every part. Nothing has to cross between parts.
All inputs are finite; a program needn't handle non-finite values.
Results may differ from the reference program's by a relative error of at most 0.007.
Values may be sent and summed in bfloat16 or wider, within the bound.
No kernel may reach another device: no remote copies, remote signals or barrier semaphores. Data moves between devices by JAX's collectives and lax.ppermute only.
A program may use at most 128 MiB of HBM per device.

```python
import math
import jax
import jax.numpy as jnp
from jax import lax

D = 4096
HEADS = 32
HEAD_DIM = 64
GROUPS = 8
STATE = 128
W_INNER = 2048
BLOCK = 128
TAPS = 3
TOK_DEV = 768
TOKENS = 12288
CTX = 512


def draw_decay_log(key, part):
    first, second, third = jax.random.split(key, 3)
    chain_len = TOKENS + CTX
    slow = jax.random.uniform(first, (2, HEADS), jnp.float32, math.log(2.0 / chain_len), math.log(10.0 / chain_len))
    fast = jax.random.uniform(second, (2, HEADS), jnp.float32, math.log(0.5), math.log(2.0))
    picks = jax.random.randint(third, (2, HEADS), 0, 2)
    chosen = jnp.where(picks == 1, fast, slow)
    return chosen


def draw_decay_extra(key, part):
    first, second, third = jax.random.split(key, 3)
    span_count = TOKENS // TOK_DEV
    low_end, high_end = (0.1, 1.2)
    rate = jnp.exp(jax.random.uniform(first, (2, HEADS, span_count), jnp.float32, math.log(low_end), math.log(high_end))) / TOKENS
    equilibrium_memory = jnp.repeat(rate, TOK_DEV, axis=2)
    spots = jax.random.randint(second, (2, HEADS, 4), 0, TOKENS)
    stack_level_index = jax.random.uniform(third, (2, HEADS, 4), jnp.float32, math.log(0.5), math.log(0.8))
    places = lax.iota(jnp.int32, TOKENS)
    agreeing_tally = places[None, None, None, :] == spots[..., None]
    latent_block_tally = jnp.sum(jnp.where(agreeing_tally, stack_level_index[..., None], 0.0), axis=2)
    return latent_block_tally - equilibrium_memory


def level_of(rng, dims, shards, smallest, largest):
    factor_of, own = 1.0, jax.random.fold_in(rng, 6)
    for dim, blocks in shards:
        steps = jnp.exp(jax.random.uniform(jax.random.fold_in(own, dim), (blocks,), jnp.float32, smallest / len(shards), largest / len(shards)))
        factor_of = factor_of * jnp.repeat(steps, dims[dim] // blocks).reshape([-1 if axis == dim else 1 for axis in range(len(dims))])
    return factor_of


def bell_draw(stream_key, dims, spread, most, pieces=(), kind=jnp.bfloat16):
    level = level_of(stream_key, dims, pieces, -0.22, 0.18) if pieces else 1.0
    entries = jax.random.normal(stream_key, dims, jnp.float32) * spread * level
    return jnp.minimum(jnp.maximum(entries, -most), most).astype(kind)


def setup_inputs(seed: int = 0, part: int = 0) -> dict:
    arg_keys = jax.random.split(jax.random.key(seed), 22)
    part_splits = jax.random.split(jax.random.fold_in(arg_keys[21], part), 22)
    return {
        "latent": bell_draw(part_splits[0], (TOKENS, D), 1.0, 6.0, ((0, 32),)),
        "context": bell_draw(part_splits[1], (CTX, D), 1.0, 6.0, ((0, 16),)),
        "condition": bell_draw(part_splits[2], (D,), 1.0, 6.0),
        "context_condition": bell_draw(arg_keys[3], (D,), 1.0, 6.0),
        "shift_weight": bell_draw(arg_keys[4], (D, D), D ** -0.5, 0.09375, ((0, 16), (1, 8))),
        "scale_weight": bell_draw(arg_keys[5], (D, D), D ** -0.5, 0.09375, ((0, 16), (1, 8))),
        "gate_weight": bell_draw(arg_keys[6], (D, D), D ** -0.5, 0.09375, ((0, 16), (1, 8))),
        "norm_gain": jnp.clip(1.0 + 0.18 * jax.random.normal(arg_keys[7], (D,), jnp.float32), 0.1, 1.9),
        "out_gate_weight": bell_draw(arg_keys[8], (D, W_INNER), D ** -0.5, 0.09375, ((1, 8),)),
        "signal_weight": bell_draw(arg_keys[9], (D, W_INNER), D ** -0.5, 0.09375, ((1, 8),)),
        "writer_weight": bell_draw(arg_keys[10], (D, GROUPS * STATE), D ** -0.5, 0.09375, ((1, 8),)),
        "reader_matrix": bell_draw(arg_keys[11], (D, GROUPS * STATE), D ** -0.5, 0.09375, ((1, 8),)),
        "step_weight": bell_draw(arg_keys[12], (2, D, HEADS), D ** -0.5, 0.09375, ((2, 8),)),
        "signal_taps": bell_draw(arg_keys[13], (TAPS, W_INNER), TAPS ** -0.5, 3.5, ((1, 8),), jnp.float32),
        "writer_taps": bell_draw(arg_keys[14], (TAPS, GROUPS * STATE), TAPS ** -0.5, 3.5, ((1, 8),), jnp.float32),
        "reader_taps": bell_draw(arg_keys[15], (TAPS, GROUPS * STATE), TAPS ** -0.5, 3.5, ((1, 8),), jnp.float32),
        "step_bias": jnp.clip(-4.5 + 2.0 * jax.random.uniform(arg_keys[16], (2, HEADS), jnp.float32) ** level_of(arg_keys[16], (2, HEADS), ((1, 8),), -0.2, 0.2), -4.5, -2.5),
        "decay_log": draw_decay_log(jax.random.fold_in(arg_keys[21], 71), part),
        "decay_extra": draw_decay_extra(jax.random.fold_in(jax.random.fold_in(arg_keys[21], part), 71), part),
        "group_gain": jnp.clip(1.0 + 0.18 * jax.random.normal(arg_keys[19], (W_INNER,), jnp.float32), 0.1, 1.9),
        "output_weight": bell_draw(arg_keys[20], (W_INNER, D), W_INNER ** -0.5, 0.125, ((1, 8),)),
    }


EPSILON = 1e-06
HIGHEST = lax.Precision.HIGHEST

def modulate(rows, norm_gain, shift_vec, scale_vec):
    values = rows.astype(jnp.float32)
    normed = values * lax.rsqrt(lax.optimization_barrier(jnp.mean(values * values, axis=-1, keepdims=True)) + EPSILON) * norm_gain
    return (normed * (1.0 + scale_vec) + shift_vec).astype(jnp.bfloat16)

def centred_conv(padded, conv_taps, length):
    running = jnp.zeros((length, padded.shape[1]), jnp.float32)
    for offset in range(conv_taps.shape[0]):
        running = running + conv_taps[offset] * padded[offset:offset + length].astype(jnp.float32)
    return jax.nn.silu(running)

def project_rows(hidden, signal_weight, writer_weight, reader_matrix, step_weight):
    raw_cols = jnp.concatenate([jnp.dot(hidden, signal_weight, preferred_element_type=jnp.float32), jnp.dot(hidden, writer_weight, preferred_element_type=jnp.float32), jnp.dot(hidden, reader_matrix, preferred_element_type=jnp.float32)], axis=1).astype(jnp.bfloat16)
    step_in = jnp.stack([jnp.dot(hidden, step_weight[0], preferred_element_type=jnp.float32), jnp.dot(hidden, step_weight[1], preferred_element_type=jnp.float32)]).astype(jnp.bfloat16)
    return (raw_cols, step_in)

def split_mixed(conv_out, head_count, head_width, group_count, state_width):
    length = conv_out.shape[0]
    signal_end = head_count * head_width
    writer_end = signal_end + group_count * state_width
    signal = conv_out[:, :signal_end].reshape(length, head_count, head_width)
    writer = conv_out[:, signal_end:writer_end].reshape(length, group_count, state_width)
    reader = conv_out[:, writer_end:].reshape(length, group_count, state_width)
    return (signal, writer, reader)

def state_span(signal, step_size, log_decay, writer, reader, start_state, block):
    length, head_count, head_width = signal.shape
    group_count, state_width = (writer.shape[1], writer.shape[2])
    per_group = head_count // group_count
    blocks = length // block
    scaled = (signal * step_size[..., None]).reshape(blocks, block, group_count, per_group, head_width)
    cum_log = jnp.cumsum(log_decay.reshape(blocks, block, group_count, per_group), axis=1)
    writer_blk = writer.reshape(blocks, block, group_count, state_width)
    reader_blk = reader.reshape(blocks, block, group_count, state_width)
    inner_dot = jnp.einsum('bign,bjgn->bgij', reader_blk, writer_blk, precision=HIGHEST)
    moved = jnp.moveaxis(cum_log, 1, -1)
    gap_logs = moved[..., :, None] - moved[..., None, :]
    lower_mask = jnp.tril(jnp.ones((block, block), dtype=bool))
    weights = jnp.exp(jnp.where(lower_mask, gap_logs, -jnp.inf))
    in_block = jnp.einsum('bgij,bgeij,bjgep->bigep', inner_dot, weights, scaled, precision=HIGHEST)
    to_end = jnp.exp(cum_log[:, -1:] - cum_log)
    states = jnp.einsum('bjgn,bjge,bjgep->bgepn', writer_blk, to_end, scaled, precision=HIGHEST)
    block_decay = jnp.exp(cum_log[:, -1])

    def advance(running, block_item):
        state_add, decay_now = block_item
        return (running * decay_now[..., None, None] + state_add, running)
    last_state, before = lax.scan(advance, start_state.reshape(group_count, per_group, head_width, state_width), (states, block_decay))
    carried = jnp.einsum('bign,bgepn,bige->bigep', reader_blk, before, jnp.exp(cum_log), precision=HIGHEST)
    result = (in_block + carried).reshape(length, head_count, head_width)
    return (result, last_state.reshape(head_count, head_width, state_width))

def context_state(signal, row_weights, writer):
    length, head_count, head_width = signal.shape
    group_count, state_width = (writer.shape[1], writer.shape[2])
    per_group = head_count // group_count
    grouped = signal.reshape(length, group_count, per_group, head_width)
    weights = row_weights.reshape(length, group_count, per_group)
    summed = jnp.einsum('tgn,tge,tgep->gepn', writer, weights, grouped, precision=HIGHEST)
    return summed.reshape(head_count, head_width, state_width)

def group_norm(gated, group_count, group_gain):
    length = gated.shape[0]
    grouped = gated.reshape(length, group_count, -1)
    normed = grouped * lax.rsqrt(lax.optimization_barrier(jnp.mean(grouped * grouped, axis=-1, keepdims=True)) + EPSILON)
    return (normed.reshape(length, -1) * group_gain).astype(jnp.bfloat16)

def reference(latent, context, condition, context_condition, shift_weight, scale_weight, gate_weight, norm_gain, out_gate_weight, signal_weight, writer_weight, reader_matrix, step_weight, signal_taps, writer_taps, reader_taps, step_bias, decay_log, decay_extra, group_gain, output_weight):
    cond_act = jax.nn.silu(jnp.stack([condition, context_condition]).astype(jnp.float32)).astype(jnp.bfloat16)
    shift_vec = jnp.dot(cond_act, shift_weight, preferred_element_type=jnp.float32)
    scale_vec = jnp.dot(cond_act, scale_weight, preferred_element_type=jnp.float32)
    gate_vec = jnp.dot(cond_act[:1], gate_weight, preferred_element_type=jnp.float32)[0]
    hidden = modulate(latent, norm_gain, shift_vec[0], scale_vec[0])
    ctx_hidden = modulate(context, norm_gain, shift_vec[1], scale_vec[1])
    conv_taps = jnp.concatenate([signal_taps, writer_taps, reader_taps], axis=1)
    decay_rates = -jnp.exp(decay_log)[:, None, :]
    ctx_raw, ctx_step_in = project_rows(ctx_hidden, signal_weight, writer_weight, reader_matrix, step_weight)
    ctx_conv = centred_conv(jnp.pad(ctx_raw, ((1, 1), (0, 0))), conv_taps, CTX)
    ctx_signal, ctx_writer, _ = split_mixed(ctx_conv, HEADS, HEAD_DIM, GROUPS, STATE)
    prefix_stride_length = jax.nn.softplus(ctx_step_in.astype(jnp.float32) + step_bias[:, None, :])
    ctx_decay = decay_rates * prefix_stride_length
    cum_log = jnp.cumsum(ctx_decay, axis=1)
    ctx_forward = context_state(ctx_signal, jnp.exp(cum_log[0, -1:] - cum_log[0]) * prefix_stride_length[0], ctx_writer)
    ctx_backward = context_state(ctx_signal, jnp.exp(cum_log[1] - ctx_decay[1]) * prefix_stride_length[1], ctx_writer)
    gate_in = jnp.dot(hidden, out_gate_weight, preferred_element_type=jnp.float32).astype(jnp.bfloat16)
    raw_cols, step_in = project_rows(hidden, signal_weight, writer_weight, reader_matrix, step_weight)
    conv_out = centred_conv(jnp.pad(raw_cols, ((1, 1), (0, 0))), conv_taps, TOKENS)
    signal, writer, reader = split_mixed(conv_out, HEADS, HEAD_DIM, GROUPS, STATE)
    step_size = jax.nn.softplus(step_in.astype(jnp.float32) + step_bias[:, None, :])
    log_decay = decay_rates * step_size + jnp.swapaxes(decay_extra, 1, 2)
    forward_out, _ = state_span(signal, step_size[0], log_decay[0], writer, reader, ctx_forward, BLOCK)
    backward_out, _ = state_span(jnp.flip(signal, 0), jnp.flip(step_size[1], 0), jnp.flip(log_decay[1], 0), jnp.flip(writer, 0), jnp.flip(reader, 0), ctx_backward, BLOCK)
    both = (forward_out + jnp.flip(backward_out, 0)).reshape(TOKENS, -1)
    gated = both * jax.nn.silu(gate_in.astype(jnp.float32))
    normed = group_norm(gated, GROUPS, group_gain)
    mix = jnp.dot(normed, output_weight, preferred_element_type=jnp.float32)
    return (latent.astype(jnp.float32) + gate_vec * mix).astype(jnp.bfloat16)
```

```python
import functools
import jax
import jax.numpy as jnp
from jax import lax
from jax.experimental import pallas as pl
from jax.experimental.pallas import tpu as pltpu
from jax.sharding import PartitionSpec as P

STATE = 128
EPSILON = 1e-06
F32 = jnp.float32
BF16 = jnp.bfloat16
LANES = 128
I_TILE = 128
KINDS = 4
PIECES = 2
EDGES = 16
MIB = 2**20


def shifted(x, axis, by):
    n = lax.axis_size(axis)
    return lax.ppermute(x, axis, [(i, (i + by) % n) for i in range(n)])


def rounded(x):
    return x.astype(BF16).astype(F32)


def silu(x):
    return x / (1.0 + jnp.exp(-x))


def per_head(cols, base, heads, width):
    lane = lax.broadcasted_iota(jnp.int32, (cols.shape[0], LANES), 1)
    per_tile = LANES // width
    tiles = []
    for t in range(heads // per_tile):
        tile = jnp.broadcast_to(cols[:, base + t * per_tile : base + t * per_tile + 1], lane.shape)
        for e in range(1, per_tile):
            at = base + t * per_tile + e
            tile = jnp.where(lane >= e * width, cols[:, at : at + 1], tile)
        tiles.append(tile)
    return jnp.concatenate(tiles, axis=1)


def running_sums(values):
    n = values.shape[1]
    lane = lax.broadcasted_iota(jnp.int32, values.shape, 1)
    ahead, behind, k = values, values, 1
    while k < n:
        ahead = ahead + jnp.where(lane >= k, pltpu.roll(ahead, k, 1), 0.0)
        behind = behind + jnp.where(lane < n - k, pltpu.roll(behind, n - k, 1), 0.0)
        k *= 2
    return ahead, behind


def condense_body(cond, shift, scale, gate, out):
    n = out.shape[0]
    parts = jnp.concatenate(
        [
            jnp.dot(cond[...], shift[...], preferred_element_type=F32),
            jnp.dot(cond[...], scale[...], preferred_element_type=F32),
            jnp.dot(cond[...], gate[...], preferred_element_type=F32),
        ],
        axis=0,
    )
    for i in range(n):
        out[i] = parts[: out.shape[1], :]


def fold_body(got, out, gate):
    total = got[0]
    for i in range(1, got.shape[0]):
        total = total + got[i]
    for i in range(out.shape[0]):
        out[i] = total[: out.shape[1], :]
    gate[...] = total[out.shape[1] :, :]


def project_body(
    flags, own, oth, ctx, same, crossed, gain, vectors, w_gate, w_sig, w_wri, w_rea, w_step,
    taps, bias, dlog, extra,
    gate_out, sig_out, wri_out, rea_out, rows_out, cols_out, payload,
    acc, hidden, squares, pad, cpad, stpad,
    *, heads,
):
    k = pl.program_id(0)
    half = own.shape[0]
    length = 2 * half
    ctx_len = ctx.shape[0]
    n_sig = w_sig.shape[1]
    n_gate = w_gate.shape[1]
    n_state = w_wri.shape[1]
    width = n_sig // heads
    conv_w = n_sig + 2 * n_state
    dp = flags[0]

    @pl.when(k == 0)
    def _():
        acc[...] = jnp.zeros_like(acc)
        squares[...] = jnp.zeros_like(squares)

    w = jnp.concatenate([w_gate[...], w_sig[...], w_wri[...], w_rea[...], w_step[...]], axis=1)
    g0, b0 = gain[...] * (1.0 + vectors[0, 2:3, :]), vectors[0, 0:1, :]
    g1, b1 = gain[...] * (1.0 + vectors[0, 3:4, :]), vectors[0, 1:2, :]

    def take(values, scale, at):
        n = values.shape[0]
        hidden[at : at + n, :] = (values * scale).astype(BF16)
        part = values[:, :LANES] * values[:, :LANES]
        for t in range(1, values.shape[1] // LANES):
            tile = values[:, t * LANES : (t + 1) * LANES]
            part = part + tile * tile
        squares[at : at + n, :] += part

    first = dp == 0
    edges_before = jnp.where(first, crossed[...].astype(F32), same[...].astype(F32))
    edges_after = jnp.where(first, same[...].astype(F32), crossed[...].astype(F32))
    row = lax.broadcasted_iota(jnp.int32, (EDGES, own.shape[1]), 0)
    tile = jnp.zeros(row.shape, F32)
    for r, value in enumerate(
        (edges_before[1:2], edges_after[1:2], edges_before[0:1], edges_after[0:1])
    ):
        tile = jnp.where(row == r, value, tile)
    take(tile, jnp.where(row < 2, g1, g0), length + ctx_len)
    tile = jnp.zeros(row.shape, F32)
    for r, value in enumerate((b0, b0 - rounded(b0), b1, b1 - rounded(b1))):
        tile = jnp.where(row == r, value, tile)
    at = length + ctx_len + EDGES
    hidden[at : at + EDGES, :] = tile.astype(BF16)
    take(ctx[...].astype(F32), g1, length)
    take(own[...].astype(F32), g0, 0)
    take(oth[...].astype(F32), g0, half)
    acc[...] += jnp.dot(hidden[...], w, preferred_element_type=F32)

    @pl.when(k == pl.num_programs(0) - 1)
    def _():
        c0, c1 = n_gate, n_gate + conv_w
        d_model = own.shape[1] * pl.num_programs(0)
        prev_ok = jnp.where(flags[1] > 0, 0.0, 1.0)
        next_ok = jnp.where(flags[2] > 0, 0.0, 1.0)
        base = length + ctx_len + EDGES
        lat_add = acc[base : base + 1, :] + acc[base + 1 : base + 2, :]
        ctx_add = acc[base + 2 : base + 3, :] + acc[base + 3 : base + 4, :]
        scale = lax.rsqrt(
            jnp.sum(squares[...], axis=1, keepdims=True) * (1.0 / d_model) + EPSILON
        )

        def values(lo, n, cols, add):
            return rounded(acc[lo : lo + n, cols] * scale[lo : lo + n, :] + add[:, cols])

        conv_cols, step_cols = slice(c0, c1), slice(c1, c1 + 2 * heads)
        for lo, off in ((0, dp * half), (half, (1 - dp) * half)):
            off = pl.multiple_of(off, half)
            gate_out[pl.ds(off, half), :] = values(lo, half, slice(0, c0), lat_add).astype(BF16)
            pad[pl.ds(off + 8, half), :] = values(lo, half, conv_cols, lat_add)
            stpad[pl.ds(off, half), : 2 * heads] = values(lo, half, step_cols, lat_add)
        base = length + ctx_len
        pad[7:8, :] = values(base + 2, 1, conv_cols, lat_add) * prev_ok
        pad[8 + length : 9 + length, :] = values(base + 3, 1, conv_cols, lat_add) * next_ok
        cpad[8 : 8 + ctx_len, :] = values(length, ctx_len, conv_cols, ctx_add)
        cpad[7:8, :] = values(base, 1, conv_cols, ctx_add) * prev_ok
        cpad[8 + ctx_len : 9 + ctx_len, :] = values(base + 1, 1, conv_cols, ctx_add) * next_ok
        stpad[length : length + ctx_len, : 2 * heads] = values(length, ctx_len, step_cols, ctx_add)
        t0, t1, t2 = taps[0:1, :], taps[1:2, :], taps[2:3, :]
        conv = silu(
            t0 * pad[7 : 7 + length, :] + t1 * pad[8 : 8 + length, :] + t2 * pad[9 : 9 + length, :]
        )
        cconv = silu(
            t0 * cpad[7 : 7 + ctx_len, :]
            + t1 * cpad[8 : 8 + ctx_len, :]
            + t2 * cpad[9 : 9 + ctx_len, :]
        )
        sig, wri, rea = (
            conv[:, :n_sig],
            conv[:, n_sig : n_sig + n_state].astype(BF16),
            conv[:, n_sig + n_state :].astype(BF16),
        )
        sig_out[...] = sig.astype(BF16)
        wri_out[...] = wri
        rea_out[...] = rea
        csig, cwri = cconv[:, :n_sig], cconv[:, n_sig : n_sig + n_state].astype(BF16)

        both = 2 * heads
        turned = stpad[...].T[:both, :]
        lane = lax.broadcasted_iota(jnp.int32, turned.shape, 1)
        z = jnp.where(lane < length + ctx_len, turned, 0.0) + bias[...]
        step = jnp.maximum(z, 0.0) + jnp.log1p(jnp.exp(-jnp.abs(z)))
        more = jnp.concatenate([extra[...], jnp.zeros((both, LANES), F32)], axis=1)
        logs = -jnp.exp(dlog[...]) * step + more
        logs = jnp.where(lane < length + ctx_len, logs, 0.0)
        lat_step, lat_log = step[:, :length], logs[:, :length]
        ctx_step, ctx_log = step[:, length:], logs[:, length:]
        forward = lax.broadcasted_iota(jnp.int32, (both, 1), 0) < heads
        ahead, behind = running_sums(lat_log)
        cum = jnp.where(forward, ahead, behind)
        total = ahead[:, length - 1 :]
        lat_w = jnp.exp(total - cum) * lat_step
        c_ahead, _ = running_sums(ctx_log)
        c_total = c_ahead[:, LANES - 1 :]
        ctx_w = jnp.exp(jnp.where(forward, c_total - c_ahead, c_ahead - ctx_log)) * ctx_step
        rows_out[:both, :] = cum
        rows_out[both:, :] = lat_step
        cols = jnp.concatenate([cum, lat_w, jnp.zeros((LANES - 2 * both, length), F32)], axis=0).T
        ctx_cols = jnp.concatenate([ctx_w, jnp.zeros((LANES - both, LANES), F32)], axis=0).T
        cols_out[...] = cols
        contract = (((0,), (0,)), ((), ()))
        for direction in range(2):
            lhs = (sig * per_head(cols, both + direction * heads, heads, width)).astype(BF16)
            state = lax.dot_general(lhs, wri, contract, preferred_element_type=F32)
            part = n_sig // payload.shape[0]
            kind = direction * part
            payload[:, kind : kind + part, :] = state.reshape(-1, part, n_state).astype(BF16)
            lhs = csig * per_head(ctx_cols[:ctx_len, :], direction * heads, heads, width)
            state = lax.dot_general(lhs.astype(BF16), cwri, contract, preferred_element_type=F32)
            kind = (2 + direction) * part
            payload[:, kind : kind + part, :] = state.reshape(-1, part, n_state).astype(BF16)
        tail = payload.shape[1] - KINDS * part
        row = lax.broadcasted_iota(jnp.int32, (tail, LANES), 0)
        pieces = []
        for value in (total, c_total):
            high = rounded(value)
            pieces.append((high, value - high))
        per_slice = payload.shape[0] // heads
        for h in range(heads):
            tile = jnp.zeros((tail, LANES), F32)
            for kind in range(KINDS):
                at = (kind % 2) * heads + h
                for piece in range(PIECES):
                    value = pieces[kind // 2][piece][at : at + 1, :]
                    tile = jnp.where(row == kind * PIECES + piece, value, tile)
            for e in range(per_slice):
                payload[h * per_slice + e, KINDS * part :, :] = tile.astype(BF16)


def chain_body(got, out, *, part):
    spans = got.shape[0]

    def decay(i, kind):
        at = KINDS * part + kind * PIECES
        value = got[i, at : at + 1, :].astype(F32)
        for piece in range(1, PIECES):
            value = value + got[i, at + piece : at + piece + 1, :].astype(F32)
        return jnp.exp(value)

    def added(i, kind):
        return got[i, kind * part : (kind + 1) * part, :].astype(F32)

    for direction, order in ((0, range(spans)), (1, range(spans - 1, -1, -1))):
        state = jnp.zeros((part, got.shape[2]), F32)
        for i in order:
            state = decay(i, 2 + direction) * state + added(i, 2 + direction)
        for i in order:
            out[i, direction * part : (direction + 1) * part, :] = state.astype(BF16)
            state = decay(i, direction) * state + added(i, direction)


def inside_body(rea, wri, sig, rows, cols, out, *, heads):
    length = wri.shape[0]
    width = sig.shape[1] // heads
    block = rea.shape[0]
    start = pl.program_id(0) * block
    score = lax.dot_general(
        rea[...], wri[...], (((1,), (1,)), ((), ())), preferred_element_type=F32
    )
    i = start + lax.broadcasted_iota(jnp.int32, (block, length), 0)
    j = lax.broadcasted_iota(jnp.int32, (block, length), 1)
    below = i >= j
    above = i <= j
    for h in range(heads):
        b = heads + h
        gap = jnp.where(
            below, cols[:, h : h + 1] - rows[h : h + 1, :], cols[:, b : b + 1] - rows[b : b + 1, :]
        )
        size = jnp.where(below, rows[2 * heads + h : 2 * heads + h + 1, :], 0.0) + jnp.where(
            above, rows[2 * heads + b : 2 * heads + b + 1, :], 0.0
        )
        weights = (jnp.exp(gap) * size * score).astype(BF16)
        out[:, h * width : (h + 1) * width] = jnp.dot(
            weights, sig[:, h * width : (h + 1) * width], preferred_element_type=F32
        )


def finish_body(starts, rea, cols, inside, gate, gain, out, *, heads):
    spans, rows, state = starts.shape
    part = rows // 2
    n_sig = inside.shape[1]
    width = n_sig // heads
    contract = (((1,), (1,)), ((), ()))
    mixed = inside[...]
    decays = jnp.exp(cols[...])
    for direction in range(2):
        begin = starts[:, direction * part : (direction + 1) * part, :].reshape(n_sig, state)
        carried = lax.dot_general(rea[...], begin, contract, preferred_element_type=F32)
        mixed = mixed + carried * per_head(decays, direction * heads, heads, width)
    gated = mixed * silu(gate[...].astype(F32))
    scale = lax.rsqrt(jnp.mean(gated * gated, axis=-1, keepdims=True) + EPSILON)
    out[...] = (gated * scale * gain[...]).astype(BF16)


def output_body(where, *refs, count):
    blocks, (weight, own, oth, gate), out = refs[:count], refs[count : count + 4], refs[-1]
    n = blocks[0].shape[1]
    total = None
    for b, block in enumerate(blocks):
        at = pl.multiple_of(where[2 + b] * n, n)
        term = jnp.dot(block[...], weight[pl.ds(at, n), :], preferred_element_type=F32)
        total = term if total is None else total + term
    tiles = pl.num_programs(0) // 2
    mine = jnp.where(pl.program_id(0) // tiles == where[0], 1.0, 0.0)
    rest = own[...].astype(F32) * mine + oth[...].astype(F32) * (1.0 - mine)
    out[...] = (rest + gate[...] * total).astype(BF16)


def whole(shape):
    return pl.BlockSpec(shape, lambda *_: (0,) * len(shape))


def shaped(shape, dtype):
    return pltpu.HBM(shape, dtype)


def placed(*arrays):
    return [pltpu.with_memory_space_constraint(a, pltpu.HBM) for a in arrays]


def in_vmem(*arrays):
    return [pltpu.with_memory_space_constraint(a, pltpu.VMEM) for a in arrays]


def on_device(
    latent, context, condition, context_condition, shift_weight, scale_weight, gate_weight,
    norm_gain, out_gate_weight, signal_weight, writer_weight, reader_matrix, step_weight,
    signal_taps, writer_taps, reader_taps, step_bias, decay_log, decay_extra, group_gain,
    output_weight,
):
    sp, tp, dp = lax.axis_index("sp"), lax.axis_index("tp"), lax.axis_index("dp")
    n_sp, n_tp, n_dp = lax.axis_size("sp"), lax.axis_size("tp"), lax.axis_size("dp")
    half, d_model = latent.shape
    length = half * n_dp
    ctx_len = context.shape[0]
    heads = step_bias.shape[1]
    n_sig = signal_weight.shape[1]
    n_gate = out_gate_weight.shape[1]
    n_state = writer_weight.shape[1]
    n_out = output_weight.shape[1]

    rows_here, cols_here = shift_weight.shape
    cond_act = jax.nn.silu(jnp.stack([condition, context_condition]).astype(F32)).astype(BF16)
    own_rows = lax.dynamic_slice_in_dim(cond_act, sp * rows_here, rows_here, 1)
    parts = pl.pallas_call(
        condense_body,
        out_shape=shaped((n_sp, 5, cols_here), F32),
        compiler_params=pltpu.CompilerParams(vmem_limit_bytes=8 * MIB),
        name="condense",
    )(own_rows, *placed(shift_weight, scale_weight, gate_weight))
    latent, context, sent = lax.optimization_barrier((latent, context, parts))
    sums = lax.all_to_all(sent, "sp", split_axis=0, concat_axis=0, tiled=True)
    vectors, gate_vec = pl.pallas_call(
        fold_body,
        out_shape=(
            shaped((n_tp * n_dp, 4, cols_here), F32),
            shaped((1, cols_here), F32),
        ),
        compiler_params=pltpu.CompilerParams(vmem_limit_bytes=8 * MIB),
        name="fold",
    )(sums)
    vectors = lax.all_to_all(vectors, ("tp", "dp"), split_axis=0, concat_axis=0, tiled=True)

    oth = shifted(latent, "dp", 1)
    edge = jnp.where(
        dp == 1,
        jnp.concatenate([latent[-1:], context[-1:]]),
        jnp.concatenate([latent[:1], context[:1]]),
    )
    pairs = {0: [], 1: []}
    for s in range(n_sp):
        for flip in pairs:
            if s + 1 < n_sp:
                pairs[flip].append((2 * s + 1, 2 * (s + 1) + 1 - flip))
            if s:
                pairs[flip].append((2 * s, 2 * (s - 1) + flip))
    same = lax.ppermute(edge, ("sp", "dp"), pairs[0])
    crossed = lax.ppermute(edge, ("sp", "dp"), pairs[1])

    flags = jnp.stack([dp, sp == 0, sp == n_sp - 1]).astype(jnp.int32)
    taps = jnp.concatenate([signal_taps, writer_taps, reader_taps], axis=1)
    steps = jnp.moveaxis(step_weight, 0, 1).reshape(d_model, 2 * heads)
    extra = decay_extra.reshape(2 * heads, length)
    n_all = n_gate + n_sig + 2 * n_state + 2 * heads
    n_rows = length + ctx_len + 2 * EDGES
    part = n_sig // n_sp
    tail = KINDS * PIECES
    conv_w = n_sig + 2 * n_state
    tile = lambda rows: pl.BlockSpec((rows, cols_here), lambda k, *_: (0, k))
    down = lambda cols: pl.BlockSpec((cols_here, cols), lambda k, *_: (k, 0))
    outs = (
        shaped((length, n_gate), BF16),
        shaped((length, n_sig), BF16),
        shaped((length, n_state), BF16),
        shaped((length, n_state), BF16),
        shaped((4 * heads, length), F32),
        shaped((length, LANES), F32),
        shaped((n_sp, KINDS * part + tail, n_state), BF16),
    )
    gate_in, signal, writer, reader, rows, cols, payload = pl.pallas_call(
        functools.partial(project_body, heads=heads),
        out_shape=outs,
        grid_spec=pltpu.PrefetchScalarGridSpec(
            num_scalar_prefetch=1,
            grid=(d_model // cols_here,),
            in_specs=[
                tile(half), tile(half), tile(ctx_len), tile(2), tile(2), tile(1),
                pl.BlockSpec((1, 4, cols_here), lambda k, *_: (k, 0, 0)),
                down(n_gate), down(n_sig), down(n_state), down(n_state), down(2 * heads),
                whole((3, conv_w)), whole((2 * heads, 1)), whole((2 * heads, 1)),
                whole((2 * heads, length)),
            ],
            out_specs=[whole(o.shape) for o in outs],
            scratch_shapes=[
                pltpu.VMEM((n_rows, n_all), F32),
                pltpu.VMEM((n_rows, cols_here), BF16),
                pltpu.VMEM((n_rows, LANES), F32),
                pltpu.VMEM((length + 16, conv_w), F32),
                pltpu.VMEM((ctx_len + 16, conv_w), F32),
                pltpu.VMEM((length + LANES, LANES), F32),
            ],
        ),
        compiler_params=pltpu.CompilerParams(
            dimension_semantics=("arbitrary",), vmem_limit_bytes=28 * MIB
        ),
        cost_estimate=pl.CostEstimate(
            flops=2 * n_rows * d_model * n_all, transcendentals=0,
            bytes_accessed=2 * d_model * (n_rows + n_all),
        ),
        name="project",
    )(
        flags, *placed(latent), oth, *placed(context), same, crossed, norm_gain.reshape(1, -1), vectors,
        *placed(out_gate_weight, signal_weight, writer_weight, reader_matrix, steps),
        taps, step_bias.reshape(-1, 1), decay_log.reshape(-1, 1), extra,
    )

    got = lax.all_to_all(payload, "sp", split_axis=0, concat_axis=0, tiled=True)
    row_block = lambda cols_: pl.BlockSpec((I_TILE, cols_), lambda i: (i, 0))
    inside = pl.pallas_call(
        functools.partial(inside_body, heads=heads),
        out_shape=shaped((length, n_sig), F32),
        grid=(length // I_TILE,),
        in_specs=[
            row_block(n_state), whole((length, n_state)), whole((length, n_sig)),
            whole((4 * heads, length)), row_block(LANES),
        ],
        out_specs=row_block(n_sig),
        compiler_params=pltpu.CompilerParams(vmem_limit_bytes=16 * MIB),
        cost_estimate=pl.CostEstimate(
            flops=2 * length * length * (n_state + 4 * n_sig),
            transcendentals=heads * length * length,
            bytes_accessed=4 * length * n_sig,
        ),
        name="inside",
    )(*placed(reader, writer, signal, rows, cols))
    starts = pl.pallas_call(
        functools.partial(chain_body, part=part),
        out_shape=shaped((n_sp, 2 * part, n_state), BF16),
        compiler_params=pltpu.CompilerParams(vmem_limit_bytes=4 * MIB),
        name="chain",
    )(got)
    starts = lax.all_to_all(starts, "sp", split_axis=0, concat_axis=0, tiled=True)
    normed = pl.pallas_call(
        functools.partial(finish_body, heads=heads),
        out_shape=pltpu.VMEM((length, n_sig), BF16),
        compiler_params=pltpu.CompilerParams(vmem_limit_bytes=12 * MIB),
        name="finish",
    )(*in_vmem(starts), *placed(reader, cols, inside, gate_in), group_gain.reshape(1, -1))
    at = tp * n_dp + dp
    blocks, places = [normed], [at]
    for by in (*range(2, n_tp - 1), n_tp - 1, 1):
        blocks.append(shifted(normed, "tp", by))
        places.append((tp + n_tp - by) % n_tp * n_dp + dp)
    for one, place in list(zip(blocks, places)):
        blocks.append(shifted(one, "dp", 1))
        places.append(place - dp + 1 - dp)
    where = jnp.stack([dp, at, *places]).astype(jnp.int32)
    count = len(blocks)
    rows_out = half // 2
    return pl.pallas_call(
        functools.partial(output_body, count=count),
        out_shape=shaped((length, n_out), BF16),
        grid_spec=pltpu.PrefetchScalarGridSpec(
            num_scalar_prefetch=1,
            grid=(length // rows_out,),
            in_specs=[pl.BlockSpec((rows_out, n_sig), lambda i, w: (i, 0))] * count
            + [
                whole(output_weight.shape),
                pl.BlockSpec((rows_out, n_out), lambda i, w: (i % 2, w[1])),
                pl.BlockSpec((rows_out, n_out), lambda i, w: (i % 2, w[1])),
                whole((1, n_out)),
            ],
            out_specs=pl.BlockSpec((rows_out, n_out), lambda i, w: (i, 0)),
        ),
        compiler_params=pltpu.CompilerParams(vmem_limit_bytes=14 * MIB),
        cost_estimate=pl.CostEstimate(
            flops=2 * length * n_sig * count * n_out, transcendentals=0,
            bytes_accessed=2 * count * n_sig * (length + n_out),
        ),
        name="output",
    )(where, *in_vmem(*blocks), *placed(output_weight, latent), oth, gate_vec)


def solution(mesh):
    tensor = ("tp", "dp")
    in_specs = (
        P(("grp", "sp", "dp"), None), P(("grp", "sp"), None), P("grp"), P(),
        P("sp", tensor), P("sp", tensor), P("sp", tensor), P(),
        P(None, tensor), P(None, tensor), P(None, tensor), P(None, tensor),
        P(None, None, tensor), P(None, tensor), P(None, tensor), P(None, tensor),
        P(None, tensor), P(None, tensor), P(None, tensor, ("grp", "sp")), P(tensor),
        P(None, tensor),
    )
    return jax.shard_map(
        on_device, mesh=mesh, in_specs=in_specs, out_specs=P(("grp", "sp"), tensor),
        check_vma=False,
    )
```

```python
import functools
import jax
import jax.numpy as jnp
from jax import lax
from jax.experimental import pallas as pl
from jax.experimental.pallas import tpu as pltpu
from jax.sharding import PartitionSpec as P

STATE = 128
EPSILON = 1e-06
F32 = jnp.float32
BF16 = jnp.bfloat16
LANES = 128
I_TILE = 128
KINDS = 4
PIECES = 2
EDGES = 16
CHUNKS = 2
MIB = 2**20


def shifted(x, axis, by):
    n = lax.axis_size(axis)
    return lax.ppermute(x, axis, [(i, (i + by) % n) for i in range(n)])


def rounded(x):
    return x.astype(BF16).astype(F32)


def silu(x):
    return x / (1.0 + jnp.exp(-x))


def per_head(cols, base, heads, width):
    lane = lax.broadcasted_iota(jnp.int32, (cols.shape[0], LANES), 1)
    per_tile = LANES // width
    tiles = []
    for t in range(heads // per_tile):
        tile = jnp.broadcast_to(cols[:, base + t * per_tile : base + t * per_tile + 1], lane.shape)
        for e in range(1, per_tile):
            at = base + t * per_tile + e
            tile = jnp.where(lane >= e * width, cols[:, at : at + 1], tile)
        tiles.append(tile)
    return jnp.concatenate(tiles, axis=1)


def running_sums(values):
    n = values.shape[1]
    lane = lax.broadcasted_iota(jnp.int32, values.shape, 1)
    ahead, behind, k = values, values, 1
    while k < n:
        ahead = ahead + jnp.where(lane >= k, pltpu.roll(ahead, k, 1), 0.0)
        behind = behind + jnp.where(lane < n - k, pltpu.roll(behind, n - k, 1), 0.0)
        k *= 2
    return ahead, behind


def condense_body(where, cond, ctx_cond, shift, scale, gate, out, wide):
    rows = shift.shape[0] // LANES
    acts = []
    for c, ref in enumerate((cond, ctx_cond)):
        n = ref.shape[0]
        wide[c * n : (c + 1) * n, :] = silu(ref[...].astype(F32))
        picked = [wide[pl.ds(c * n + where[0] * rows + r, 1), :] for r in range(rows)]
        acts.append(jnp.concatenate(picked, axis=1))
    row = lax.broadcasted_iota(jnp.int32, (8, shift.shape[0]), 0)
    acts = jnp.where(row == 0, acts[0], jnp.where(row == 1, acts[1], 0.0)).astype(BF16)
    parts = jnp.concatenate(
        [
            jnp.dot(acts, shift[...], preferred_element_type=F32)[:2, :],
            jnp.dot(acts, scale[...], preferred_element_type=F32)[:2, :],
            jnp.dot(acts, gate[...], preferred_element_type=F32)[:1, :],
        ],
        axis=0,
    )
    for i in range(out.shape[0]):
        out[i] = parts


def fold_body(got, out, gate):
    total = got[0]
    for i in range(1, got.shape[0]):
        total = total + got[i]
    for i in range(out.shape[0]):
        out[i] = total[: out.shape[1], :]
    gate[...] = total[out.shape[1] :, :]


def project_body(
    flags, own, oth, ctx, same, crossed, gain, vectors, w_gate, w_sig, w_wri, w_rea,
    w_step, taps, bias, dlog, extra,
    gate_out, sig_out, wri_out, rea_out, rows_out, cols_out, payload,
    acc, squares, pad, cpad, stpad, *hiddens,
    heads,
):
    k = pl.program_id(0)
    half = own.shape[0]
    length = 2 * half
    ctx_len = ctx.shape[0]
    n_sig = w_sig.shape[1]
    n_gate = w_gate.shape[1]
    n_state = w_wri.shape[1]
    width = n_sig // heads
    conv_w = n_sig + 2 * n_state
    dp = flags[0]
    first = dp == 0
    wide = hiddens[0].shape[1]

    @pl.when(k == 0)
    def _():
        acc[...] = jnp.zeros_like(acc)
        squares[...] = jnp.zeros_like(squares)

    def take(hidden, values, scale, at):
        n = values.shape[0]
        hidden[at : at + n, :] = (values * scale).astype(BF16)
        part = values[:, :LANES] * values[:, :LANES]
        for t in range(1, values.shape[1] // LANES):
            tile = values[:, t * LANES : (t + 1) * LANES]
            part = part + tile * tile
        squares[at : at + n, :] += part

    for c, hidden in enumerate(hiddens):
        cut = slice(c * wide, (c + 1) * wide)
        w = jnp.concatenate([r[cut, :] for r in (w_gate, w_sig, w_wri, w_rea, w_step)], axis=1)
        g0, b0 = gain[:, cut] * (1.0 + vectors[c, 2:3, :]), vectors[c, 0:1, :]
        g1, b1 = gain[:, cut] * (1.0 + vectors[c, 3:4, :]), vectors[c, 1:2, :]
        edges = [same[:, cut].astype(F32), crossed[:, cut].astype(F32)]
        edges_before = jnp.where(first, edges[1], edges[0])
        edges_after = jnp.where(first, edges[0], edges[1])
        row = lax.broadcasted_iota(jnp.int32, (EDGES, wide), 0)
        tile = jnp.zeros(row.shape, F32)
        for r, value in enumerate(
            (edges_before[1:2], edges_after[1:2], edges_before[0:1], edges_after[0:1])
        ):
            tile = jnp.where(row == r, value, tile)
        at = length + ctx_len
        take(hidden, tile, jnp.where(row < 2, g1, g0), at)
        tile = jnp.zeros(row.shape, F32)
        for r, value in enumerate((b0, b0 - rounded(b0), b1, b1 - rounded(b1))):
            tile = jnp.where(row == r, value, tile)
        hidden[at + EDGES : at + 2 * EDGES, :] = tile.astype(BF16)
        take(hidden, ctx[:, cut].astype(F32), g1, length)
        take(hidden, own[:, cut].astype(F32), g0, 0)
        take(hidden, oth[:, cut].astype(F32), g0, half)
        acc[...] += jnp.dot(hidden[...], w, preferred_element_type=F32)

    @pl.when(k == pl.num_programs(0) - 1)
    def _():
        c0, c1 = n_gate, n_gate + conv_w
        d_model = own.shape[1] * pl.num_programs(0)
        prev_ok = jnp.where(flags[1] > 0, 0.0, 1.0)
        next_ok = jnp.where(flags[2] > 0, 0.0, 1.0)
        base = length + ctx_len + EDGES
        lat_add = acc[base : base + 1, :] + acc[base + 1 : base + 2, :]
        ctx_add = acc[base + 2 : base + 3, :] + acc[base + 3 : base + 4, :]
        scale = lax.rsqrt(
            jnp.sum(squares[...], axis=1, keepdims=True) * (1.0 / d_model) + EPSILON
        )

        def values(lo, n, cols, add):
            return rounded(acc[lo : lo + n, cols] * scale[lo : lo + n, :] + add[:, cols])

        conv_cols, step_cols = slice(c0, c1), slice(c1, c1 + 2 * heads)
        for lo, off in ((0, dp * half), (half, (1 - dp) * half)):
            off = pl.multiple_of(off, half)
            gate_out[pl.ds(off, half), :] = values(lo, half, slice(0, c0), lat_add).astype(BF16)
            pad[pl.ds(off + 8, half), :] = values(lo, half, conv_cols, lat_add)
            stpad[pl.ds(off, half), : 2 * heads] = values(lo, half, step_cols, lat_add)
        base = length + ctx_len
        pad[7:8, :] = values(base + 2, 1, conv_cols, lat_add) * prev_ok
        pad[8 + length : 9 + length, :] = values(base + 3, 1, conv_cols, lat_add) * next_ok
        cpad[8 : 8 + ctx_len, :] = values(length, ctx_len, conv_cols, ctx_add)
        cpad[7:8, :] = values(base, 1, conv_cols, ctx_add) * prev_ok
        cpad[8 + ctx_len : 9 + ctx_len, :] = values(base + 1, 1, conv_cols, ctx_add) * next_ok
        stpad[length : length + ctx_len, : 2 * heads] = values(length, ctx_len, step_cols, ctx_add)
        t0, t1, t2 = taps[0:1, :], taps[1:2, :], taps[2:3, :]
        conv = silu(
            t0 * pad[7 : 7 + length, :] + t1 * pad[8 : 8 + length, :] + t2 * pad[9 : 9 + length, :]
        )
        cconv = silu(
            t0 * cpad[7 : 7 + ctx_len, :]
            + t1 * cpad[8 : 8 + ctx_len, :]
            + t2 * cpad[9 : 9 + ctx_len, :]
        )
        sig, wri, rea = (
            conv[:, :n_sig],
            conv[:, n_sig : n_sig + n_state].astype(BF16),
            conv[:, n_sig + n_state :].astype(BF16),
        )
        sig_out[...] = sig.astype(BF16)
        wri_out[...] = wri
        rea_out[...] = rea
        csig, cwri = cconv[:, :n_sig], cconv[:, n_sig : n_sig + n_state].astype(BF16)

        both = 2 * heads
        turned = stpad[...].T[:both, :]
        lane = lax.broadcasted_iota(jnp.int32, turned.shape, 1)
        z = jnp.where(lane < length + ctx_len, turned, 0.0) + bias[...]
        step = jnp.maximum(z, 0.0) + jnp.log1p(jnp.exp(-jnp.abs(z)))
        more = jnp.concatenate([extra[...], jnp.zeros((both, LANES), F32)], axis=1)
        logs = -jnp.exp(dlog[...]) * step + more
        logs = jnp.where(lane < length + ctx_len, logs, 0.0)
        lat_step, lat_log = step[:, :length], logs[:, :length]
        ctx_step, ctx_log = step[:, length:], logs[:, length:]
        forward = lax.broadcasted_iota(jnp.int32, (both, 1), 0) < heads
        ahead, behind = running_sums(lat_log)
        cum = jnp.where(forward, ahead, behind)
        total = ahead[:, length - 1 :]
        lat_w = jnp.exp(total - cum) * lat_step
        c_ahead, _ = running_sums(ctx_log)
        c_total = c_ahead[:, LANES - 1 :]
        ctx_w = jnp.exp(jnp.where(forward, c_total - c_ahead, c_ahead - ctx_log)) * ctx_step
        rows_out[:both, :] = cum
        rows_out[both:, :] = lat_step
        cols = jnp.concatenate([cum, lat_w, jnp.zeros((LANES - 2 * both, length), F32)], axis=0).T
        ctx_cols = jnp.concatenate([ctx_w, jnp.zeros((LANES - both, LANES), F32)], axis=0).T
        cols_out[...] = cols
        contract = (((0,), (0,)), ((), ()))
        for direction in range(2):
            lhs = (sig * per_head(cols, both + direction * heads, heads, width)).astype(BF16)
            state = lax.dot_general(lhs, wri, contract, preferred_element_type=F32)
            part = n_sig // payload.shape[0]
            kind = direction * part
            payload[:, kind : kind + part, :] = state.reshape(-1, part, n_state).astype(BF16)
            lhs = csig * per_head(ctx_cols[:ctx_len, :], direction * heads, heads, width)
            state = lax.dot_general(lhs.astype(BF16), cwri, contract, preferred_element_type=F32)
            kind = (2 + direction) * part
            payload[:, kind : kind + part, :] = state.reshape(-1, part, n_state).astype(BF16)
        tail = payload.shape[1] - KINDS * part
        row = lax.broadcasted_iota(jnp.int32, (tail, LANES), 0)
        pieces = []
        for value in (total, c_total):
            high = rounded(value)
            pieces.append((high, value - high))
        per_slice = payload.shape[0] // heads
        for h in range(heads):
            tile = jnp.zeros((tail, LANES), F32)
            for kind in range(KINDS):
                at = (kind % 2) * heads + h
                for piece in range(PIECES):
                    value = pieces[kind // 2][piece][at : at + 1, :]
                    tile = jnp.where(row == kind * PIECES + piece, value, tile)
            for e in range(per_slice):
                payload[h * per_slice + e, KINDS * part :, :] = tile.astype(BF16)


def chain_body(got, out, *, part):
    spans = got.shape[0]

    def decay(i, kind):
        at = KINDS * part + kind * PIECES
        value = got[i, at : at + 1, :].astype(F32)
        for piece in range(1, PIECES):
            value = value + got[i, at + piece : at + piece + 1, :].astype(F32)
        return jnp.exp(value)

    def added(i, kind):
        return got[i, kind * part : (kind + 1) * part, :].astype(F32)

    for direction, order in ((0, range(spans)), (1, range(spans - 1, -1, -1))):
        state = jnp.zeros((part, got.shape[2]), F32)
        for i in order:
            state = decay(i, 2 + direction) * state + added(i, 2 + direction)
        for i in order:
            out[i, direction * part : (direction + 1) * part, :] = state.astype(BF16)
            state = decay(i, direction) * state + added(i, direction)


def inside_body(rea, wri, sig, rows, cols, out, *, heads):
    length = wri.shape[0]
    width = sig.shape[1] // heads
    block = rea.shape[0]
    start = pl.program_id(0) * block
    score = lax.dot_general(
        rea[...], wri[...], (((1,), (1,)), ((), ())), preferred_element_type=F32
    )
    i = start + lax.broadcasted_iota(jnp.int32, (block, length), 0)
    j = lax.broadcasted_iota(jnp.int32, (block, length), 1)
    below = i >= j
    above = i <= j
    for h in range(heads):
        b = heads + h
        gap = jnp.where(
            below, cols[:, h : h + 1] - rows[h : h + 1, :], cols[:, b : b + 1] - rows[b : b + 1, :]
        )
        size = jnp.where(below, rows[2 * heads + h : 2 * heads + h + 1, :], 0.0) + jnp.where(
            above, rows[2 * heads + b : 2 * heads + b + 1, :], 0.0
        )
        weights = (jnp.exp(gap) * size * score).astype(BF16)
        out[:, h * width : (h + 1) * width] = jnp.dot(
            weights, sig[:, h * width : (h + 1) * width], preferred_element_type=F32
        )


def finish_body(starts, rea, cols, inside, gate, gain, out, *, heads):
    spans, rows, state = starts.shape
    part = rows // 2
    n_sig = inside.shape[1]
    width = n_sig // heads
    contract = (((1,), (1,)), ((), ()))
    mixed = inside[...]
    decays = jnp.exp(cols[...])
    for direction in range(2):
        begin = starts[:, direction * part : (direction + 1) * part, :].reshape(n_sig, state)
        carried = lax.dot_general(rea[...], begin, contract, preferred_element_type=F32)
        mixed = mixed + carried * per_head(decays, direction * heads, heads, width)
    gated = mixed * silu(gate[...].astype(F32))
    scale = lax.rsqrt(jnp.mean(gated * gated, axis=-1, keepdims=True) + EPSILON)
    out[...] = (gated * scale * gain[...]).astype(BF16)


def output_body(where, *refs, count):
    blocks, (weight, own, oth, gate, out) = refs[:count], refs[count : count + 5]
    left, right, rest, done, sems = refs[count + 5 :]
    length, n = blocks[0].shape
    n_out = out.shape[1]
    half = own.shape[0]
    parts = length // half
    column = pl.multiple_of(where[1] * n_out, n_out)
    copies = []

    def start(source, target):
        copies.append(pltpu.make_async_copy(source, target, sems.at[len(copies)]))
        copies[-1].start()

    for b in range(count):
        at = pl.multiple_of(where[2 + b] * n, n)
        start(weight.at[pl.ds(at, n), :], right.at[b * n : (b + 1) * n, :])
        start(blocks[b].at[:half, :], left.at[:half, b * n : (b + 1) * n])
    start(own.at[:, pl.ds(column, n_out)], rest.at[0])
    start(oth.at[:, pl.ds(column, n_out)], rest.at[1])
    for p in range(1, parts):
        for b in range(count):
            start(
                blocks[b].at[p * half : (p + 1) * half, :],
                left.at[p * half : (p + 1) * half, b * n : (b + 1) * n],
            )
    first = 2 * count + 2
    for copy in copies[:first]:
        copy.wait()
    writes = []
    for p in range(parts):
        for copy in copies[first + (p - 1) * count : first + p * count] if p else []:
            copy.wait()
        rows = slice(p * half, (p + 1) * half)
        total = jnp.dot(left[rows, :], right[...], preferred_element_type=F32)
        mine = jnp.where(where[0] == p, 1.0, 0.0)
        base = rest[0].astype(F32) * mine + rest[1].astype(F32) * (1.0 - mine)
        done[rows, :] = (base + gate[...] * total).astype(BF16)
        writes.append(pltpu.make_async_copy(done.at[rows, :], out.at[rows, :], sems.at[p]))
        writes[-1].start()
    for write in writes:
        write.wait()


def whole(shape):
    return pl.BlockSpec(shape, lambda *_: (0,) * len(shape))


def shaped(shape, dtype):
    return pltpu.HBM(shape, dtype)


def placed(*arrays):
    return [pltpu.with_memory_space_constraint(a, pltpu.HBM) for a in arrays]


def in_vmem(*arrays):
    return [pltpu.with_memory_space_constraint(a, pltpu.VMEM) for a in arrays]


def on_device(
    latent, context, condition, context_condition, shift_weight, scale_weight, gate_weight,
    norm_gain, out_gate_weight, signal_weight, writer_weight, reader_matrix, step_weight,
    signal_taps, writer_taps, reader_taps, step_bias, decay_log, decay_extra, group_gain,
    output_weight,
):
    sp, tp, dp = lax.axis_index("sp"), lax.axis_index("tp"), lax.axis_index("dp")
    n_sp, n_tp, n_dp = lax.axis_size("sp"), lax.axis_size("tp"), lax.axis_size("dp")
    half, d_model = latent.shape
    length = half * n_dp
    ctx_len = context.shape[0]
    heads = step_bias.shape[1]
    n_sig = signal_weight.shape[1]
    n_gate = out_gate_weight.shape[1]
    n_state = writer_weight.shape[1]
    n_out = output_weight.shape[1]

    cols_here = shift_weight.shape[1]
    small = lambda n: pltpu.CompilerParams(vmem_limit_bytes=n * MIB)
    parts = pl.pallas_call(
        condense_body,
        out_shape=shaped((n_sp, 5, cols_here), F32),
        grid_spec=pltpu.PrefetchScalarGridSpec(
            num_scalar_prefetch=1,
            grid=(1,),
            in_specs=[whole((d_model // LANES, LANES))] * 2 + [whole(shift_weight.shape)] * 3,
            out_specs=whole((n_sp, 5, cols_here)),
            scratch_shapes=[pltpu.VMEM((2 * d_model // LANES, LANES), F32)],
        ),
        compiler_params=small(8),
        name="condense",
    )(
        sp.astype(jnp.int32)[None],
        *placed(condition.reshape(-1, LANES), context_condition.reshape(-1, LANES)),
        *placed(shift_weight, scale_weight, gate_weight),
    )
    latent, context, sent = lax.optimization_barrier((latent, context, parts))
    sums = lax.all_to_all(sent, "sp", split_axis=0, concat_axis=0, tiled=True)
    taps = jnp.concatenate([signal_taps, writer_taps, reader_taps], axis=1)
    steps = jnp.moveaxis(step_weight, 0, 1).reshape(d_model, 2 * heads)
    extra = decay_extra.reshape(2 * heads, length)
    bias, rates = step_bias.reshape(-1, 1), decay_log.reshape(-1, 1)
    sums, taps, steps, extra, bias, rates = lax.optimization_barrier(
        (sums, taps, steps, extra, bias, rates)
    )
    vectors, gate_vec = pl.pallas_call(
        fold_body,
        out_shape=(
            shaped((n_tp * n_dp, 4, cols_here), F32),
            shaped((1, cols_here), F32),
        ),
        compiler_params=pltpu.CompilerParams(vmem_limit_bytes=8 * MIB),
        name="fold",
    )(sums)
    vectors = lax.all_to_all(vectors, ("tp", "dp"), split_axis=0, concat_axis=0, tiled=True)

    oth = shifted(latent, "dp", 1)
    edge = jnp.where(
        dp == 1,
        jnp.concatenate([latent[-1:], context[-1:]]),
        jnp.concatenate([latent[:1], context[:1]]),
    )
    pairs = {0: [], 1: []}
    for s in range(n_sp):
        for flip in pairs:
            if s + 1 < n_sp:
                pairs[flip].append((2 * s + 1, 2 * (s + 1) + 1 - flip))
            if s:
                pairs[flip].append((2 * s, 2 * (s - 1) + flip))
    same = lax.ppermute(edge, ("sp", "dp"), pairs[0])
    crossed = lax.ppermute(edge, ("sp", "dp"), pairs[1])

    flags = jnp.stack([dp, sp == 0, sp == n_sp - 1]).astype(jnp.int32)
    n_all = n_gate + n_sig + 2 * n_state + 2 * heads
    n_rows = length + ctx_len + 2 * EDGES
    part = n_sig // n_sp
    tail = KINDS * PIECES
    conv_w = n_sig + 2 * n_state
    k_tile = CHUNKS * cols_here
    tile = lambda rows: pl.BlockSpec((rows, k_tile), lambda k, *_: (0, k))
    down = lambda cols: pl.BlockSpec((k_tile, cols), lambda k, *_: (k, 0))
    outs = (
        shaped((length, n_gate), BF16),
        shaped((length, n_sig), BF16),
        shaped((length, n_state), BF16),
        shaped((length, n_state), BF16),
        shaped((4 * heads, length), F32),
        shaped((length, LANES), F32),
        shaped((n_sp, KINDS * part + tail, n_state), BF16),
    )
    gate_in, signal, writer, reader, rows, cols, payload = pl.pallas_call(
        functools.partial(project_body, heads=heads),
        out_shape=outs,
        grid_spec=pltpu.PrefetchScalarGridSpec(
            num_scalar_prefetch=1,
            grid=(d_model // k_tile,),
            in_specs=[
                tile(half), tile(half), tile(ctx_len), tile(2), tile(2),
                tile(1),
                pl.BlockSpec((CHUNKS, 4, cols_here), lambda k, *_: (k, 0, 0)),
                down(n_gate), down(n_sig), down(n_state), down(n_state), down(2 * heads),
                whole((3, conv_w)), whole((2 * heads, 1)), whole((2 * heads, 1)),
                whole((2 * heads, length)),
            ],
            out_specs=[whole(o.shape) for o in outs],
            scratch_shapes=[
                pltpu.VMEM((n_rows, n_all), F32),
                pltpu.VMEM((n_rows, LANES), F32),
                pltpu.VMEM((length + 16, conv_w), F32),
                pltpu.VMEM((ctx_len + 16, conv_w), F32),
                pltpu.VMEM((length + LANES, LANES), F32),
            ]
            + [pltpu.VMEM((n_rows, cols_here), BF16)] * CHUNKS,
        ),
        compiler_params=pltpu.CompilerParams(
            dimension_semantics=("arbitrary",), vmem_limit_bytes=28 * MIB
        ),
        cost_estimate=pl.CostEstimate(
            flops=2 * n_rows * d_model * n_all, transcendentals=0,
            bytes_accessed=2 * d_model * (n_rows + n_all),
        ),
        name="project",
    )(
        flags, *placed(latent), oth, *placed(context), same, crossed, norm_gain.reshape(1, -1), vectors,
        *placed(out_gate_weight, signal_weight, writer_weight, reader_matrix, steps),
        taps, bias, rates, extra,
    )

    got = lax.all_to_all(payload, "sp", split_axis=0, concat_axis=0, tiled=True)
    row_block = lambda cols_: pl.BlockSpec((I_TILE, cols_), lambda i: (i, 0))
    inside = pl.pallas_call(
        functools.partial(inside_body, heads=heads),
        out_shape=shaped((length, n_sig), F32),
        grid=(length // I_TILE,),
        in_specs=[
            row_block(n_state), whole((length, n_state)), whole((length, n_sig)),
            whole((4 * heads, length)), row_block(LANES),
        ],
        out_specs=row_block(n_sig),
        compiler_params=pltpu.CompilerParams(vmem_limit_bytes=16 * MIB),
        cost_estimate=pl.CostEstimate(
            flops=2 * length * length * (n_state + 4 * n_sig),
            transcendentals=heads * length * length,
            bytes_accessed=4 * length * n_sig,
        ),
        name="inside",
    )(*placed(reader, writer, signal, rows, cols))
    got, inside = lax.optimization_barrier((got, inside))
    starts = pl.pallas_call(
        functools.partial(chain_body, part=part),
        out_shape=shaped((n_sp, 2 * part, n_state), BF16),
        compiler_params=pltpu.CompilerParams(vmem_limit_bytes=4 * MIB),
        name="chain",
    )(got)
    starts = lax.all_to_all(starts, "sp", split_axis=0, concat_axis=0, tiled=True)
    normed = pl.pallas_call(
        functools.partial(finish_body, heads=heads),
        out_shape=shaped((length, n_sig), BF16),
        compiler_params=pltpu.CompilerParams(vmem_limit_bytes=12 * MIB),
        name="finish",
    )(starts, *placed(reader, cols, inside, gate_in), group_gain.reshape(1, -1))
    at = tp * n_dp + dp
    blocks, places = placed(normed), [at]
    for by in (n_tp - 1, 1, *range(2, n_tp - 1)):
        blocks.append(shifted(normed, "tp", by))
        places.append((tp + n_tp - by) % n_tp * n_dp + dp)
    for one, place in list(zip(blocks, places)):
        blocks.append(shifted(one, "dp", 1))
        places.append(place - dp + 1 - dp)
    where = jnp.stack([dp, at, *places]).astype(jnp.int32)
    count = len(blocks)
    anywhere = pl.BlockSpec(memory_space=pl.ANY)
    return pl.pallas_call(
        functools.partial(output_body, count=count),
        out_shape=shaped((length, n_out), BF16),
        grid_spec=pltpu.PrefetchScalarGridSpec(
            num_scalar_prefetch=1,
            grid=(1,),
            in_specs=[anywhere] * (count + 3) + [whole((1, n_out))],
            out_specs=anywhere,
            scratch_shapes=[
                pltpu.VMEM((length, n_sig * count), BF16),
                pltpu.VMEM((n_sig * count, n_out), BF16),
                pltpu.VMEM((2, half, n_out), BF16),
                pltpu.VMEM((length, n_out), BF16),
                pltpu.SemaphoreType.DMA((n_dp * (count + 1) + count + 1,)),
            ],
        ),
        compiler_params=small(24),
        name="output",
    )(where, *placed(*blocks), *placed(output_weight, latent), oth, gate_vec)


def solution(mesh):
    tensor = ("tp", "dp")
    in_specs = (
        P(("grp", "sp", "dp"), None), P(("grp", "sp"), None), P("grp"), P(),
        P("sp", tensor), P("sp", tensor), P("sp", tensor), P(),
        P(None, tensor), P(None, tensor), P(None, tensor), P(None, tensor),
        P(None, None, tensor), P(None, tensor), P(None, tensor), P(None, tensor),
        P(None, tensor), P(None, tensor), P(None, tensor, ("grp", "sp")), P(tensor),
        P(None, tensor),
    )
    return jax.shard_map(
        on_device, mesh=mesh, in_specs=in_specs, out_specs=P(("grp", "sp"), tensor),
        check_vma=False,
    )
```

```python
import functools
import jax
import jax.numpy as jnp
from jax import lax
from jax.experimental import pallas as pl
from jax.experimental.pallas import tpu as pltpu
from jax.sharding import PartitionSpec as P

STATE = 128
EPSILON = 1e-06
F32 = jnp.float32
BF16 = jnp.bfloat16
LANES = 128
I_TILE = 128
KINDS = 4
PIECES = 2
EDGES = 16
CHUNKS = 2
MIB = 2**20


def shifted(x, axis, by):
    n = lax.axis_size(axis)
    return lax.ppermute(x, axis, [(i, (i + by) % n) for i in range(n)])


def rounded(x):
    return x.astype(BF16).astype(F32)


def silu(x):
    return x / (1.0 + jnp.exp(-x))


def per_head(cols, base, heads, width):
    lane = lax.broadcasted_iota(jnp.int32, (cols.shape[0], LANES), 1)
    per_tile = LANES // width
    tiles = []
    for t in range(heads // per_tile):
        tile = jnp.broadcast_to(cols[:, base + t * per_tile : base + t * per_tile + 1], lane.shape)
        for e in range(1, per_tile):
            at = base + t * per_tile + e
            tile = jnp.where(lane >= e * width, cols[:, at : at + 1], tile)
        tiles.append(tile)
    return jnp.concatenate(tiles, axis=1)


def running_sums(values):
    n = values.shape[1]
    lane = lax.broadcasted_iota(jnp.int32, values.shape, 1)
    ahead, behind, k = values, values, 1
    while k < n:
        ahead = ahead + jnp.where(lane >= k, pltpu.roll(ahead, k, 1), 0.0)
        behind = behind + jnp.where(lane < n - k, pltpu.roll(behind, n - k, 1), 0.0)
        k *= 2
    return ahead, behind


def condense_body(where, cond, ctx_cond, shift, scale, gate, out, wide, turned):
    rows = shift.shape[0] // LANES
    acts = []
    for c, ref in enumerate((cond, ctx_cond)):
        n = ref.shape[0]
        wide[c * n : (c + 1) * n, :] = silu(ref[...].astype(F32))
        picked = [wide[pl.ds(c * n + where[0] * rows + r, 1), :] for r in range(rows)]
        acts.append(jnp.concatenate(picked, axis=1))
    row = lax.broadcasted_iota(jnp.int32, (8, shift.shape[0]), 0)
    acts = jnp.where(row == 0, acts[0], jnp.where(row == 1, acts[1], 0.0)).astype(BF16)
    at = 0
    for weight, n in ((shift, 2), (scale, 2), (gate, 1)):
        part = jnp.dot(acts, weight[...], preferred_element_type=F32)
        for r in range(n):
            for t in range(part.shape[1] // LANES):
                turned[at : at + 1, :] = part[r : r + 1, t * LANES : (t + 1) * LANES]
                at += 1
    sent = turned[: out.shape[1], :].astype(BF16)
    for i in range(out.shape[0]):
        out[i] = sent


def fold_body(got, out, gate):
    total = got[0].astype(F32)
    for i in range(1, got.shape[0]):
        total = total + got[i].astype(F32)
    n = out.shape[1]
    for i in range(out.shape[0]):
        out[i] = total[:n, :]
    gate[...] = jnp.concatenate(
        [total[r : r + 1, :] for r in range(n, n + gate.shape[1] // LANES)], axis=1
    )


def project_body(
    flags, own, oth, ctx, same, crossed, gain, vectors, w_gate, w_sig, w_wri, w_rea,
    w_step, sig_taps, wri_taps, rea_taps, bias, rates, extra,
    gate_out, sig_out, wri_out, rea_out, rows_out, cols_out, payload,
    acc, acc_step, squares, pad, cpad, stpad, small, *hiddens,
    heads,
):
    k = pl.program_id(0)
    half = own.shape[0]
    length = 2 * half
    ctx_len = ctx.shape[0]
    n_sig = w_sig.shape[1]
    n_gate = w_gate.shape[1]
    n_state = w_wri.shape[1]
    width = n_sig // heads
    conv_w = n_sig + 2 * n_state
    dp = flags[0]
    first = dp == 0
    wide = hiddens[0].shape[1]

    @pl.when(k == 0)
    def _():
        acc[...] = jnp.zeros_like(acc)
        acc_step[...] = jnp.zeros_like(acc_step)
        squares[...] = jnp.zeros_like(squares)

    def take(hidden, values, scale, at):
        n = values.shape[0]
        hidden[at : at + n, :] = (values * scale).astype(BF16)
        part = values[:, :LANES] * values[:, :LANES]
        for t in range(1, values.shape[1] // LANES):
            tile = values[:, t * LANES : (t + 1) * LANES]
            part = part + tile * tile
        squares[at : at + n, :] += part

    for c, hidden in enumerate(hiddens):
        cut = slice(c * wide, (c + 1) * wide)
        w = jnp.concatenate([r[cut, :] for r in (w_gate, w_sig, w_wri, w_rea)], axis=1)
        for direction in range(2):
            small[direction * heads : (direction + 1) * heads, :] = w_step[
                direction, :, cut
            ].astype(F32)
        per = wide // LANES
        b0, b1, g0, g1 = (
            jnp.concatenate(
                [vectors[c, r * per + t : r * per + t + 1, :] for t in range(per)], axis=1
            )
            for r in range(4)
        )
        g0, g1 = gain[:, cut] * (1.0 + g0), gain[:, cut] * (1.0 + g1)
        edges = [same[:, cut].astype(F32), crossed[:, cut].astype(F32)]
        edges_before = jnp.where(first, edges[1], edges[0])
        edges_after = jnp.where(first, edges[0], edges[1])
        row = lax.broadcasted_iota(jnp.int32, (EDGES, wide), 0)
        tile = jnp.zeros(row.shape, F32)
        for r, value in enumerate(
            (edges_before[1:2], edges_after[1:2], edges_before[0:1], edges_after[0:1])
        ):
            tile = jnp.where(row == r, value, tile)
        at = length + ctx_len
        take(hidden, tile, jnp.where(row < 2, g1, g0), at)
        tile = jnp.zeros(row.shape, F32)
        for r, value in enumerate((b0, b0 - rounded(b0), b1, b1 - rounded(b1))):
            tile = jnp.where(row == r, value, tile)
        hidden[at + EDGES : at + 2 * EDGES, :] = tile.astype(BF16)
        take(hidden, ctx[:, cut].astype(F32), g1, length)
        take(hidden, own[:, cut].astype(F32), g0, 0)
        take(hidden, oth[:, cut].astype(F32), g0, half)
        acc[...] += jnp.dot(hidden[...], w, preferred_element_type=F32)
        acc_step[...] += lax.dot_general(
            hidden[...], small[...].astype(BF16), (((1,), (1,)), ((), ())),
            preferred_element_type=F32,
        )

    @pl.when(k == pl.num_programs(0) - 1)
    def _():
        c0, c1 = n_gate, n_gate + conv_w
        d_model = own.shape[1] * pl.num_programs(0)
        prev_ok = jnp.where(flags[1] > 0, 0.0, 1.0)
        next_ok = jnp.where(flags[2] > 0, 0.0, 1.0)
        base = length + ctx_len + EDGES
        scale = lax.rsqrt(
            jnp.sum(squares[...], axis=1, keepdims=True) * (1.0 / d_model) + EPSILON
        )

        def values(lo, n, cols, is_ctx=0, source=acc):
            at = base + 2 * is_ctx
            add = source[at : at + 1, cols] + source[at + 1 : at + 2, cols]
            return rounded(source[lo : lo + n, cols] * scale[lo : lo + n, :] + add)

        conv_cols, step_cols = slice(c0, c1), slice(0, 2 * heads)
        for lo, off in ((0, dp * half), (half, (1 - dp) * half)):
            off = pl.multiple_of(off, half)
            gate_out[pl.ds(off, half), :] = values(lo, half, slice(0, c0)).astype(BF16)
            pad[pl.ds(off + 8, half), :] = values(lo, half, conv_cols)
            stpad[pl.ds(off, half), : 2 * heads] = values(lo, half, step_cols, 0, acc_step)
        edge = length + ctx_len
        pad[7:8, :] = values(edge + 2, 1, conv_cols) * prev_ok
        pad[8 + length : 9 + length, :] = values(edge + 3, 1, conv_cols) * next_ok
        cpad[8 : 8 + ctx_len, :] = values(length, ctx_len, conv_cols, 1)
        cpad[7:8, :] = values(edge, 1, conv_cols, 1) * prev_ok
        cpad[8 + ctx_len : 9 + ctx_len, :] = values(edge + 1, 1, conv_cols, 1) * next_ok
        stpad[length : length + ctx_len, : 2 * heads] = values(length, ctx_len, step_cols, 1, acc_step)
        taps = jnp.concatenate([sig_taps[...], wri_taps[...], rea_taps[...]], axis=1)
        t0, t1, t2 = taps[0:1, :], taps[1:2, :], taps[2:3, :]
        conv = silu(
            t0 * pad[7 : 7 + length, :] + t1 * pad[8 : 8 + length, :] + t2 * pad[9 : 9 + length, :]
        )
        cconv = silu(
            t0 * cpad[7 : 7 + ctx_len, :]
            + t1 * cpad[8 : 8 + ctx_len, :]
            + t2 * cpad[9 : 9 + ctx_len, :]
        )
        sig, wri, rea = (
            conv[:, :n_sig],
            conv[:, n_sig : n_sig + n_state].astype(BF16),
            conv[:, n_sig + n_state :].astype(BF16),
        )
        sig_out[...] = sig.astype(BF16)
        wri_out[...] = wri
        rea_out[...] = rea
        blank = jnp.zeros((LANES - ctx_len, conv_w), F32)
        cconv = jnp.concatenate([cconv, blank], axis=0)
        csig, cwri = cconv[:, :n_sig], cconv[:, n_sig : n_sig + n_state].astype(BF16)

        both = 2 * heads
        turned = stpad[...].T[:both, :]
        lane = lax.broadcasted_iota(jnp.int32, turned.shape, 1)
        which = lax.broadcasted_iota(jnp.int32, (both, 1), 0)
        shift, rate = jnp.zeros((both, 1), F32), jnp.zeros((both, 1), F32)
        for r in range(both):
            d, h = divmod(r, heads)
            shift = jnp.where(which == r, bias[d : d + 1, h : h + 1], shift)
            rate = jnp.where(which == r, rates[d : d + 1, h : h + 1], rate)
        z = jnp.where(lane < length + ctx_len, turned, 0.0) + shift
        step = jnp.maximum(z, 0.0) + jnp.log1p(jnp.exp(-jnp.abs(z)))
        for direction in range(2):
            rows_out[direction * heads : (direction + 1) * heads, :] = extra[direction]
        more = jnp.concatenate([rows_out[:both, :], jnp.zeros((both, LANES), F32)], axis=1)
        logs = -jnp.exp(rate) * step + more
        logs = jnp.where(lane < length + ctx_len, logs, 0.0)
        lat_step, lat_log = step[:, :length], logs[:, :length]
        ctx_step, ctx_log = step[:, length:], logs[:, length:]
        forward = lax.broadcasted_iota(jnp.int32, (both, 1), 0) < heads
        ahead, behind = running_sums(lat_log)
        cum = jnp.where(forward, ahead, behind)
        total = ahead[:, length - 1 :]
        lat_w = jnp.exp(total - cum) * lat_step
        c_ahead, _ = running_sums(ctx_log)
        c_total = c_ahead[:, LANES - 1 :]
        ctx_w = jnp.exp(jnp.where(forward, c_total - c_ahead, c_ahead - ctx_log)) * ctx_step
        rows_out[:both, :] = cum
        rows_out[both:, :] = lat_step
        cols_out[...] = jnp.concatenate([cum, jnp.zeros((LANES - both, length), F32)], axis=0).T
        part = n_sig // payload.shape[0]
        kind = 0
        for values_t, weights, other in ((sig.T, lat_w, wri), (csig.T, ctx_w, cwri)):
            for direction in range(2):
                lhs = jnp.concatenate(
                    [
                        values_t[h * width : (h + 1) * width, :]
                        * weights[direction * heads + h : direction * heads + h + 1, :]
                        for h in range(heads)
                    ],
                    axis=0,
                ).astype(BF16)
                state = jnp.dot(lhs, other, preferred_element_type=F32)
                payload[:, kind : kind + part, :] = state.reshape(-1, part, n_state).astype(BF16)
                kind += part
        tail = payload.shape[1] - KINDS * part
        row = lax.broadcasted_iota(jnp.int32, (tail, LANES), 0)
        pieces = []
        for value in (total, c_total):
            high = rounded(value)
            pieces.append((high, value - high))
        per_slice = payload.shape[0] // heads
        for h in range(heads):
            tile = jnp.zeros((tail, LANES), F32)
            for kind in range(KINDS):
                at = (kind % 2) * heads + h
                for piece in range(PIECES):
                    value = pieces[kind // 2][piece][at : at + 1, :]
                    tile = jnp.where(row == kind * PIECES + piece, value, tile)
            for e in range(per_slice):
                payload[h * per_slice + e, KINDS * part :, :] = tile.astype(BF16)


def chain_body(got, out, *, part):
    spans = got.shape[0]

    def decay(i, kind):
        at = KINDS * part + kind * PIECES
        value = got[i, at : at + 1, :].astype(F32)
        for piece in range(1, PIECES):
            value = value + got[i, at + piece : at + piece + 1, :].astype(F32)
        return jnp.exp(value)

    def added(i, kind):
        return got[i, kind * part : (kind + 1) * part, :].astype(F32)

    for direction, order in ((0, range(spans)), (1, range(spans - 1, -1, -1))):
        state = jnp.zeros((part, got.shape[2]), F32)
        for i in order:
            state = decay(i, 2 + direction) * state + added(i, 2 + direction)
        for i in order:
            out[i, direction * part : (direction + 1) * part, :] = state.astype(BF16)
            state = decay(i, direction) * state + added(i, direction)


def inside_body(rea, wri, sig, rows, cols, out, *, heads):
    length = wri.shape[0]
    width = sig.shape[1] // heads
    block = rea.shape[0]
    start = pl.program_id(0) * block
    score = lax.dot_general(
        rea[...], wri[...], (((1,), (1,)), ((), ())), preferred_element_type=F32
    )
    i = start + lax.broadcasted_iota(jnp.int32, (block, length), 0)
    j = lax.broadcasted_iota(jnp.int32, (block, length), 1)
    below = i >= j
    above = i <= j
    for h in range(heads):
        b = heads + h
        gap = jnp.where(
            below, cols[:, h : h + 1] - rows[h : h + 1, :], cols[:, b : b + 1] - rows[b : b + 1, :]
        )
        size = jnp.where(below, rows[2 * heads + h : 2 * heads + h + 1, :], 0.0) + jnp.where(
            above, rows[2 * heads + b : 2 * heads + b + 1, :], 0.0
        )
        weights = (jnp.exp(gap) * size * score).astype(BF16)
        out[:, h * width : (h + 1) * width] = jnp.dot(
            weights, sig[:, h * width : (h + 1) * width], preferred_element_type=F32
        )


def finish_body(starts, rea, cols, inside, gate, gain, out, *, heads):
    spans, rows, state = starts.shape
    part = rows // 2
    n_sig = inside.shape[1]
    width = n_sig // heads
    contract = (((1,), (1,)), ((), ()))
    mixed = inside[...]
    decays = jnp.exp(cols[...])
    for direction in range(2):
        begin = starts[:, direction * part : (direction + 1) * part, :].reshape(n_sig, state)
        carried = lax.dot_general(rea[...], begin, contract, preferred_element_type=F32)
        mixed = mixed + carried * per_head(decays, direction * heads, heads, width)
    gated = mixed * silu(gate[...].astype(F32))
    scale = lax.rsqrt(jnp.mean(gated * gated, axis=-1, keepdims=True) + EPSILON)
    out[...] = (gated * scale * gain[...]).astype(BF16)


def output_body(where, *refs, count):
    blocks, (weight, own, oth, gate, out) = refs[:count], refs[count : count + 5]
    left, right, rest, done, sems = refs[count + 5 :]
    length, n = blocks[0].shape
    n_out = out.shape[1]
    half = own.shape[0]
    parts = length // half
    column = pl.multiple_of(where[1] * n_out, n_out)
    copies = []

    def start(source, target):
        copies.append(pltpu.make_async_copy(source, target, sems.at[len(copies)]))
        copies[-1].start()

    for b in range(count):
        at = pl.multiple_of(where[2 + b] * n, n)
        start(weight.at[pl.ds(at, n), :], right.at[b * n : (b + 1) * n, :])
        start(blocks[b].at[:half, :], left.at[:half, b * n : (b + 1) * n])
    start(own.at[:, pl.ds(column, n_out)], rest.at[0])
    start(oth.at[:, pl.ds(column, n_out)], rest.at[1])
    for p in range(1, parts):
        for b in range(count):
            start(
                blocks[b].at[p * half : (p + 1) * half, :],
                left.at[p * half : (p + 1) * half, b * n : (b + 1) * n],
            )
    first = 2 * count + 2
    for copy in copies[:first]:
        copy.wait()
    writes = []
    for p in range(parts):
        for copy in copies[first + (p - 1) * count : first + p * count] if p else []:
            copy.wait()
        rows = slice(p * half, (p + 1) * half)
        total = jnp.dot(left[rows, :], right[...], preferred_element_type=F32)
        mine = jnp.where(where[0] == p, 1.0, 0.0)
        base = rest[0].astype(F32) * mine + rest[1].astype(F32) * (1.0 - mine)
        done[rows, :] = (base + gate[...] * total).astype(BF16)
        writes.append(pltpu.make_async_copy(done.at[rows, :], out.at[rows, :], sems.at[p]))
        writes[-1].start()
    for write in writes:
        write.wait()


def whole(shape):
    return pl.BlockSpec(shape, lambda *_: (0,) * len(shape))


def shaped(shape, dtype):
    return pltpu.HBM(shape, dtype)


def placed(*arrays):
    return [pltpu.with_memory_space_constraint(a, pltpu.HBM) for a in arrays]


def in_vmem(*arrays):
    return [pltpu.with_memory_space_constraint(a, pltpu.VMEM) for a in arrays]


def on_device(
    latent, context, condition, context_condition, shift_weight, scale_weight, gate_weight,
    norm_gain, out_gate_weight, signal_weight, writer_weight, reader_matrix, step_weight,
    signal_taps, writer_taps, reader_taps, step_bias, decay_log, decay_extra, group_gain,
    output_weight,
):
    sp, tp, dp = lax.axis_index("sp"), lax.axis_index("tp"), lax.axis_index("dp")
    n_sp, n_tp, n_dp = lax.axis_size("sp"), lax.axis_size("tp"), lax.axis_size("dp")
    half, d_model = latent.shape
    length = half * n_dp
    ctx_len = context.shape[0]
    heads = step_bias.shape[1]
    n_sig = signal_weight.shape[1]
    n_gate = out_gate_weight.shape[1]
    n_state = writer_weight.shape[1]
    n_out = output_weight.shape[1]

    cols_here = shift_weight.shape[1]
    small = lambda n: pltpu.CompilerParams(vmem_limit_bytes=n * MIB)
    parts = pl.pallas_call(
        condense_body,
        out_shape=shaped((n_sp, 5 * cols_here // LANES, LANES), BF16),
        grid_spec=pltpu.PrefetchScalarGridSpec(
            num_scalar_prefetch=1,
            grid=(1,),
            in_specs=[whole((d_model // LANES, LANES))] * 2 + [whole(shift_weight.shape)] * 3,
            out_specs=whole((n_sp, 5 * cols_here // LANES, LANES)),
            scratch_shapes=[
                pltpu.VMEM((2 * d_model // LANES, LANES), F32),
                pltpu.VMEM((8 * cols_here // LANES, LANES), F32),
            ],
        ),
        compiler_params=small(8),
        name="condense",
    )(
        sp.astype(jnp.int32)[None],
        *placed(condition.reshape(-1, LANES), context_condition.reshape(-1, LANES)),
        *placed(shift_weight, scale_weight, gate_weight),
    )
    latent, context, sent = lax.optimization_barrier((latent, context, parts))
    sums = lax.all_to_all(sent, "sp", split_axis=0, concat_axis=0, tiled=True)
    vectors, gate_vec = pl.pallas_call(
        fold_body,
        out_shape=(
            shaped((n_tp * n_dp, 4 * cols_here // LANES, LANES), F32),
            shaped((1, cols_here), F32),
        ),
        compiler_params=pltpu.CompilerParams(vmem_limit_bytes=8 * MIB),
        name="fold",
    )(sums)
    vectors = lax.all_to_all(vectors, ("tp", "dp"), split_axis=0, concat_axis=0, tiled=True)

    oth = shifted(latent, "dp", 1)
    edge = jnp.where(
        dp == 1,
        jnp.concatenate([latent[-1:], context[-1:]]),
        jnp.concatenate([latent[:1], context[:1]]),
    )
    pairs = {0: [], 1: []}
    for s in range(n_sp):
        for flip in pairs:
            if s + 1 < n_sp:
                pairs[flip].append((2 * s + 1, 2 * (s + 1) + 1 - flip))
            if s:
                pairs[flip].append((2 * s, 2 * (s - 1) + flip))
    same = lax.ppermute(edge, ("sp", "dp"), pairs[0])
    crossed = lax.ppermute(edge, ("sp", "dp"), pairs[1])

    flags = jnp.stack([dp, sp == 0, sp == n_sp - 1]).astype(jnp.int32)
    n_all = n_gate + n_sig + 2 * n_state
    n_rows = length + ctx_len + 2 * EDGES
    part = n_sig // n_sp
    tail = KINDS * PIECES
    conv_w = n_sig + 2 * n_state
    k_tile = CHUNKS * cols_here
    tile = lambda rows: pl.BlockSpec((rows, k_tile), lambda k, *_: (0, k))
    down = lambda cols: pl.BlockSpec((k_tile, cols), lambda k, *_: (k, 0))
    outs = (
        shaped((length, n_gate), BF16),
        shaped((length, n_sig), BF16),
        shaped((length, n_state), BF16),
        shaped((length, n_state), BF16),
        shaped((4 * heads, length), F32),
        shaped((length, LANES), F32),
        shaped((n_sp, KINDS * part + tail, n_state), BF16),
    )
    gate_in, signal, writer, reader, rows, cols, payload = pl.pallas_call(
        functools.partial(project_body, heads=heads),
        out_shape=outs,
        grid_spec=pltpu.PrefetchScalarGridSpec(
            num_scalar_prefetch=1,
            grid=(d_model // k_tile,),
            in_specs=[
                tile(half), tile(half), tile(ctx_len), tile(2), tile(2),
                tile(1),
                pl.BlockSpec((CHUNKS, 4 * cols_here // LANES, LANES), lambda k, *_: (k, 0, 0)),
                down(n_gate), down(n_sig), down(n_state), down(n_state),
                pl.BlockSpec((2, heads, k_tile), lambda k, *_: (0, 0, k)),
                whole(signal_taps.shape), whole(writer_taps.shape), whole(reader_taps.shape),
                whole(step_bias.shape), whole(decay_log.shape), whole(decay_extra.shape),
            ],
            out_specs=[whole(o.shape) for o in outs],
            scratch_shapes=[
                pltpu.VMEM((n_rows, n_all), F32),
                pltpu.VMEM((n_rows, 2 * heads), F32),
                pltpu.VMEM((n_rows, LANES), F32),
                pltpu.VMEM((length + 16, conv_w), F32),
                pltpu.VMEM((ctx_len + 16, conv_w), F32),
                pltpu.VMEM((length + LANES, LANES), F32),
                pltpu.VMEM((2 * heads, cols_here), F32),
            ]
            + [pltpu.VMEM((n_rows, cols_here), BF16)] * CHUNKS,
        ),
        compiler_params=pltpu.CompilerParams(
            dimension_semantics=("arbitrary",), vmem_limit_bytes=28 * MIB
        ),
        cost_estimate=pl.CostEstimate(
            flops=2 * n_rows * d_model * n_all, transcendentals=0,
            bytes_accessed=2 * d_model * (n_rows + n_all),
        ),
        name="project",
    )(
        flags, *placed(latent), oth, *placed(context), same, crossed, *placed(norm_gain.reshape(1, -1)), vectors,
        *placed(out_gate_weight, signal_weight, writer_weight, reader_matrix),
        *placed(jnp.swapaxes(step_weight, 1, 2)), *placed(signal_taps, writer_taps, reader_taps),
        *placed(step_bias, decay_log, decay_extra),
    )

    got = lax.all_to_all(payload, "sp", split_axis=0, concat_axis=0, tiled=True)
    row_block = lambda cols_: pl.BlockSpec((I_TILE, cols_), lambda i: (i, 0))
    inside = pl.pallas_call(
        functools.partial(inside_body, heads=heads),
        out_shape=shaped((length, n_sig), F32),
        grid=(length // I_TILE,),
        in_specs=[
            row_block(n_state), whole((length, n_state)), whole((length, n_sig)),
            whole((4 * heads, length)), row_block(LANES),
        ],
        out_specs=row_block(n_sig),
        compiler_params=pltpu.CompilerParams(vmem_limit_bytes=16 * MIB),
        cost_estimate=pl.CostEstimate(
            flops=2 * length * length * (n_state + 4 * n_sig),
            transcendentals=heads * length * length,
            bytes_accessed=4 * length * n_sig,
        ),
        name="inside",
    )(*placed(reader, writer, signal, rows, cols))
    got, inside = lax.optimization_barrier((got, inside))
    starts = pl.pallas_call(
        functools.partial(chain_body, part=part),
        out_shape=shaped((n_sp, 2 * part, n_state), BF16),
        compiler_params=pltpu.CompilerParams(vmem_limit_bytes=4 * MIB),
        name="chain",
    )(got)
    starts = lax.all_to_all(starts, "sp", split_axis=0, concat_axis=0, tiled=True)
    normed = pl.pallas_call(
        functools.partial(finish_body, heads=heads),
        out_shape=shaped((length, n_sig), BF16),
        compiler_params=pltpu.CompilerParams(vmem_limit_bytes=12 * MIB),
        name="finish",
    )(starts, *placed(reader, cols, inside, gate_in), group_gain.reshape(1, -1))
    at = tp * n_dp + dp
    blocks, places = placed(normed), [at]
    for by in (n_tp - 1, 1, *range(2, n_tp - 1)):
        blocks.append(shifted(normed, "tp", by))
        places.append((tp + n_tp - by) % n_tp * n_dp + dp)
    for one, place in list(zip(blocks, places)):
        blocks.append(shifted(one, "dp", 1))
        places.append(place - dp + 1 - dp)
    where = jnp.stack([dp, at, *places]).astype(jnp.int32)
    count = len(blocks)
    anywhere = pl.BlockSpec(memory_space=pl.ANY)
    return pl.pallas_call(
        functools.partial(output_body, count=count),
        out_shape=shaped((length, n_out), BF16),
        grid_spec=pltpu.PrefetchScalarGridSpec(
            num_scalar_prefetch=1,
            grid=(1,),
            in_specs=[anywhere] * (count + 3) + [whole((1, n_out))],
            out_specs=anywhere,
            scratch_shapes=[
                pltpu.VMEM((length, n_sig * count), BF16),
                pltpu.VMEM((n_sig * count, n_out), BF16),
                pltpu.VMEM((2, half, n_out), BF16),
                pltpu.VMEM((length, n_out), BF16),
                pltpu.SemaphoreType.DMA((n_dp * (count + 1) + count + 1,)),
            ],
        ),
        compiler_params=small(24),
        name="output",
    )(where, *placed(*blocks), *placed(output_weight, latent), oth, gate_vec)


def solution(mesh):
    tensor = ("tp", "dp")
    in_specs = (
        P(("grp", "sp", "dp"), None), P(("grp", "sp"), None), P("grp"), P(),
        P("sp", tensor), P("sp", tensor), P("sp", tensor), P(),
        P(None, tensor), P(None, tensor), P(None, tensor), P(None, tensor),
        P(None, None, tensor), P(None, tensor), P(None, tensor), P(None, tensor),
        P(None, tensor), P(None, tensor), P(None, tensor, ("grp", "sp")), P(tensor),
        P(None, tensor),
    )
    return jax.shard_map(
        on_device, mesh=mesh, in_specs=in_specs, out_specs=P(("grp", "sp"), tensor),
        check_vma=False,
    )
```

```python
import functools
import jax
import jax.numpy as jnp
from jax import lax
from jax.experimental import pallas as pl
from jax.experimental.pallas import tpu as pltpu
from jax.sharding import PartitionSpec as P

STATE = 128
EPSILON = 1e-06
F32 = jnp.float32
BF16 = jnp.bfloat16
LANES = 128
I_TILE = 128
KINDS = 4
PIECES = 2
EDGES = 16
CHUNKS = 2
MIB = 2**20


def shifted(x, axis, by):
    n = lax.axis_size(axis)
    return lax.ppermute(x, axis, [(i, (i + by) % n) for i in range(n)])


def rounded(x):
    return x.astype(BF16).astype(F32)


def silu(x):
    return x / (1.0 + jnp.exp(-x))


def per_head(cols, base, heads, width):
    lane = lax.broadcasted_iota(jnp.int32, (cols.shape[0], LANES), 1)
    per_tile = LANES // width
    tiles = []
    for t in range(heads // per_tile):
        tile = jnp.broadcast_to(cols[:, base + t * per_tile : base + t * per_tile + 1], lane.shape)
        for e in range(1, per_tile):
            at = base + t * per_tile + e
            tile = jnp.where(lane >= e * width, cols[:, at : at + 1], tile)
        tiles.append(tile)
    return jnp.concatenate(tiles, axis=1)


def running_sums(values):
    n = values.shape[1]
    lane = lax.broadcasted_iota(jnp.int32, values.shape, 1)
    ahead, behind, k = values, values, 1
    while k < n:
        ahead = ahead + jnp.where(lane >= k, pltpu.roll(ahead, k, 1), 0.0)
        behind = behind + jnp.where(lane < n - k, pltpu.roll(behind, n - k, 1), 0.0)
        k *= 2
    return ahead, behind


def condense_body(where, cond, ctx_cond, shift, scale, gate, out, wide, turned):
    rows = shift.shape[0] // LANES
    acts = []
    for c, ref in enumerate((cond, ctx_cond)):
        n = ref.shape[0]
        wide[c * n : (c + 1) * n, :] = silu(ref[...].astype(F32))
        picked = [wide[pl.ds(c * n + where[0] * rows + r, 1), :] for r in range(rows)]
        acts.append(jnp.concatenate(picked, axis=1))
    row = lax.broadcasted_iota(jnp.int32, (8, shift.shape[0]), 0)
    acts = jnp.where(row == 0, acts[0], jnp.where(row == 1, acts[1], 0.0)).astype(BF16)
    at = 0
    for weight, n in ((shift, 2), (scale, 2), (gate, 1)):
        part = jnp.dot(acts, weight[...], preferred_element_type=F32)
        for r in range(n):
            for t in range(part.shape[1] // LANES):
                turned[at : at + 1, :] = part[r : r + 1, t * LANES : (t + 1) * LANES]
                at += 1
    sent = turned[: out.shape[1], :].astype(BF16)
    for i in range(out.shape[0]):
        out[i] = sent


def fold_body(got, out, gate):
    total = got[0].astype(F32)
    for i in range(1, got.shape[0]):
        total = total + got[i].astype(F32)
    n = out.shape[1]
    for i in range(out.shape[0]):
        out[i] = total[:n, :]
    gate[...] = jnp.concatenate(
        [total[r : r + 1, :] for r in range(n, n + gate.shape[1] // LANES)], axis=1
    )


def project_body(
    flags, own, oth, ctx, same, crossed, gain, vectors, w_gate, w_sig, w_wri, w_rea,
    w_step, sig_taps, wri_taps, rea_taps, bias, rates, extra,
    gate_out, sig_out, wri_out, rea_out, rows_out, cols_out, payload,
    acc, acc_step, squares, pad, cpad, stpad, small, *hiddens,
    heads,
):
    k = pl.program_id(0)
    half = own.shape[0]
    length = 2 * half
    ctx_len = ctx.shape[0]
    n_sig = w_sig.shape[1]
    n_gate = w_gate.shape[1]
    n_state = w_wri.shape[1]
    width = n_sig // heads
    conv_w = n_sig + 2 * n_state
    dp = flags[0]
    first = dp == 0
    wide = hiddens[0].shape[1]

    @pl.when(k == 0)
    def _():
        acc[...] = jnp.zeros_like(acc)
        acc_step[...] = jnp.zeros_like(acc_step)
        squares[...] = jnp.zeros_like(squares)

    def take(hidden, values, scale, at):
        n = values.shape[0]
        hidden[at : at + n, :] = (values * scale).astype(BF16)
        part = values[:, :LANES] * values[:, :LANES]
        for t in range(1, values.shape[1] // LANES):
            tile = values[:, t * LANES : (t + 1) * LANES]
            part = part + tile * tile
        squares[at : at + n, :] += part

    for c, hidden in enumerate(hiddens):
        cut = slice(c * wide, (c + 1) * wide)
        w = jnp.concatenate([r[cut, :] for r in (w_gate, w_sig, w_wri, w_rea)], axis=1)
        for direction in range(2):
            small[direction * heads : (direction + 1) * heads, :] = w_step[
                direction, :, cut
            ].astype(F32)
        per = wide // LANES
        b0, b1, g0, g1 = (
            jnp.concatenate(
                [vectors[c, r * per + t : r * per + t + 1, :] for t in range(per)], axis=1
            )
            for r in range(4)
        )
        g0, g1 = gain[:, cut] * (1.0 + g0), gain[:, cut] * (1.0 + g1)
        edges = [same[:, cut].astype(F32), crossed[:, cut].astype(F32)]
        edges_before = jnp.where(first, edges[1], edges[0])
        edges_after = jnp.where(first, edges[0], edges[1])
        row = lax.broadcasted_iota(jnp.int32, (EDGES, wide), 0)
        tile = jnp.zeros(row.shape, F32)
        for r, value in enumerate(
            (edges_before[1:2], edges_after[1:2], edges_before[0:1], edges_after[0:1])
        ):
            tile = jnp.where(row == r, value, tile)
        at = length + ctx_len
        take(hidden, tile, jnp.where(row < 2, g1, g0), at)
        tile = jnp.zeros(row.shape, F32)
        for r, value in enumerate((b0, b0 - rounded(b0), b1, b1 - rounded(b1))):
            tile = jnp.where(row == r, value, tile)
        hidden[at + EDGES : at + 2 * EDGES, :] = tile.astype(BF16)
        take(hidden, ctx[:, cut].astype(F32), g1, length)
        take(hidden, own[:, cut].astype(F32), g0, 0)
        take(hidden, oth[:, cut].astype(F32), g0, half)
        acc[...] += jnp.dot(hidden[...], w, preferred_element_type=F32)
        acc_step[...] += lax.dot_general(
            hidden[...], small[...].astype(BF16), (((1,), (1,)), ((), ())),
            preferred_element_type=F32,
        )

    @pl.when(k == pl.num_programs(0) - 1)
    def _():
        c0, c1 = n_gate, n_gate + conv_w
        d_model = own.shape[1] * pl.num_programs(0)
        prev_ok = jnp.where(flags[1] > 0, 0.0, 1.0)
        next_ok = jnp.where(flags[2] > 0, 0.0, 1.0)
        base = length + ctx_len + EDGES
        scale = lax.rsqrt(
            jnp.sum(squares[...], axis=1, keepdims=True) * (1.0 / d_model) + EPSILON
        )

        def values(lo, n, cols, is_ctx=0, source=acc):
            at = base + 2 * is_ctx
            add = source[at : at + 1, cols] + source[at + 1 : at + 2, cols]
            return rounded(source[lo : lo + n, cols] * scale[lo : lo + n, :] + add)

        conv_cols, step_cols = slice(c0, c1), slice(0, 2 * heads)
        for lo, off in ((0, dp * half), (half, (1 - dp) * half)):
            off = pl.multiple_of(off, half)
            gate_out[pl.ds(off, half), :] = values(lo, half, slice(0, c0)).astype(BF16)
            pad[pl.ds(off + 8, half), :] = values(lo, half, conv_cols)
            stpad[pl.ds(off, half), : 2 * heads] = values(lo, half, step_cols, 0, acc_step)
        edge = length + ctx_len
        pad[7:8, :] = values(edge + 2, 1, conv_cols) * prev_ok
        pad[8 + length : 9 + length, :] = values(edge + 3, 1, conv_cols) * next_ok
        cpad[8 : 8 + ctx_len, :] = values(length, ctx_len, conv_cols, 1)
        cpad[7:8, :] = values(edge, 1, conv_cols, 1) * prev_ok
        cpad[8 + ctx_len : 9 + ctx_len, :] = values(edge + 1, 1, conv_cols, 1) * next_ok
        stpad[length : length + ctx_len, : 2 * heads] = values(length, ctx_len, step_cols, 1, acc_step)
        taps = jnp.concatenate([sig_taps[...], wri_taps[...], rea_taps[...]], axis=1)
        t0, t1, t2 = taps[0:1, :], taps[1:2, :], taps[2:3, :]
        conv = silu(
            t0 * pad[7 : 7 + length, :] + t1 * pad[8 : 8 + length, :] + t2 * pad[9 : 9 + length, :]
        )
        cconv = silu(
            t0 * cpad[7 : 7 + ctx_len, :]
            + t1 * cpad[8 : 8 + ctx_len, :]
            + t2 * cpad[9 : 9 + ctx_len, :]
        )
        sig, wri, rea = (
            conv[:, :n_sig],
            conv[:, n_sig : n_sig + n_state].astype(BF16),
            conv[:, n_sig + n_state :].astype(BF16),
        )
        sig_out[...] = sig.astype(BF16)
        wri_out[...] = wri
        rea_out[...] = rea
        blank = jnp.zeros((LANES - ctx_len, conv_w), F32)
        cconv = jnp.concatenate([cconv, blank], axis=0)
        csig, cwri = cconv[:, :n_sig], cconv[:, n_sig : n_sig + n_state].astype(BF16)

        both = 2 * heads
        turned = stpad[...].T[:both, :]
        lane = lax.broadcasted_iota(jnp.int32, turned.shape, 1)
        which = lax.broadcasted_iota(jnp.int32, (both, 1), 0)
        shift, rate = jnp.zeros((both, 1), F32), jnp.zeros((both, 1), F32)
        for r in range(both):
            d, h = divmod(r, heads)
            shift = jnp.where(which == r, bias[d : d + 1, h : h + 1], shift)
            rate = jnp.where(which == r, rates[d : d + 1, h : h + 1], rate)
        z = jnp.where(lane < length + ctx_len, turned, 0.0) + shift
        step = jnp.maximum(z, 0.0) + jnp.log1p(jnp.exp(-jnp.abs(z)))
        for direction in range(2):
            rows_out[direction * heads : (direction + 1) * heads, :] = extra[direction]
        more = jnp.concatenate([rows_out[:both, :], jnp.zeros((both, LANES), F32)], axis=1)
        logs = -jnp.exp(rate) * step + more
        logs = jnp.where(lane < length + ctx_len, logs, 0.0)
        lat_step, lat_log = step[:, :length], logs[:, :length]
        ctx_step, ctx_log = step[:, length:], logs[:, length:]
        forward = lax.broadcasted_iota(jnp.int32, (both, 1), 0) < heads
        ahead, behind = running_sums(lat_log)
        cum = jnp.where(forward, ahead, behind)
        total = ahead[:, length - 1 :]
        lat_w = jnp.exp(total - cum) * lat_step
        c_ahead, _ = running_sums(ctx_log)
        c_total = c_ahead[:, LANES - 1 :]
        ctx_w = jnp.exp(jnp.where(forward, c_total - c_ahead, c_ahead - ctx_log)) * ctx_step
        rows_out[:both, :] = cum
        rows_out[both:, :] = lat_step
        cols_out[...] = jnp.concatenate([cum, jnp.zeros((LANES - both, length), F32)], axis=0).T
        part = n_sig // payload.shape[0]
        kind = 0
        for values_t, weights, other in ((sig.T, lat_w, wri), (csig.T, ctx_w, cwri)):
            for direction in range(2):
                lhs = jnp.concatenate(
                    [
                        values_t[h * width : (h + 1) * width, :]
                        * weights[direction * heads + h : direction * heads + h + 1, :]
                        for h in range(heads)
                    ],
                    axis=0,
                ).astype(BF16)
                state = jnp.dot(lhs, other, preferred_element_type=F32)
                payload[:, kind : kind + part, :] = state.reshape(-1, part, n_state).astype(BF16)
                kind += part
        tail = payload.shape[1] - KINDS * part
        row = lax.broadcasted_iota(jnp.int32, (tail, LANES), 0)
        pieces = []
        for value in (total, c_total):
            high = rounded(value)
            pieces.append((high, value - high))
        per_slice = payload.shape[0] // heads
        for h in range(heads):
            tile = jnp.zeros((tail, LANES), F32)
            for kind in range(KINDS):
                at = (kind % 2) * heads + h
                for piece in range(PIECES):
                    value = pieces[kind // 2][piece][at : at + 1, :]
                    tile = jnp.where(row == kind * PIECES + piece, value, tile)
            for e in range(per_slice):
                payload[h * per_slice + e, KINDS * part :, :] = tile.astype(BF16)


def chain_body(got, out, *, part):
    spans = got.shape[0]

    def decay(i, kind):
        at = KINDS * part + kind * PIECES
        value = got[i, at : at + 1, :].astype(F32)
        for piece in range(1, PIECES):
            value = value + got[i, at + piece : at + piece + 1, :].astype(F32)
        return jnp.exp(value)

    def added(i, kind):
        return got[i, kind * part : (kind + 1) * part, :].astype(F32)

    for direction, order in ((0, range(spans)), (1, range(spans - 1, -1, -1))):
        state = jnp.zeros((part, got.shape[2]), F32)
        for i in order:
            state = decay(i, 2 + direction) * state + added(i, 2 + direction)
        for i in order:
            out[i, direction * part : (direction + 1) * part, :] = state.astype(BF16)
            state = decay(i, direction) * state + added(i, direction)


def inside_body(rea, wri, sig, rows, cols, out, *, heads):
    length = wri.shape[0]
    width = sig.shape[1] // heads
    block = rea.shape[0]
    start = pl.program_id(0) * block
    score = lax.dot_general(
        rea[...], wri[...], (((1,), (1,)), ((), ())), preferred_element_type=F32
    )
    i = start + lax.broadcasted_iota(jnp.int32, (block, length), 0)
    j = lax.broadcasted_iota(jnp.int32, (block, length), 1)
    below = i >= j
    above = i <= j
    for h in range(heads):
        b = heads + h
        gap = jnp.where(
            below, cols[:, h : h + 1] - rows[h : h + 1, :], cols[:, b : b + 1] - rows[b : b + 1, :]
        )
        size = jnp.where(below, rows[2 * heads + h : 2 * heads + h + 1, :], 0.0) + jnp.where(
            above, rows[2 * heads + b : 2 * heads + b + 1, :], 0.0
        )
        weights = (jnp.exp(gap) * size * score).astype(BF16)
        out[:, h * width : (h + 1) * width] = jnp.dot(
            weights, sig[:, h * width : (h + 1) * width], preferred_element_type=F32
        )


def finish_body(starts, rea, cols, inside, gate, gain, *outs, heads):
    spans, rows, state = starts.shape
    part = rows // 2
    n_sig = inside.shape[1]
    width = n_sig // heads
    contract = (((1,), (1,)), ((), ()))
    mixed = inside[...]
    decays = jnp.exp(cols[...])
    for direction in range(2):
        begin = starts[:, direction * part : (direction + 1) * part, :].reshape(n_sig, state)
        carried = lax.dot_general(rea[...], begin, contract, preferred_element_type=F32)
        mixed = mixed + carried * per_head(decays, direction * heads, heads, width)
    gated = mixed * silu(gate[...].astype(F32))
    scale = lax.rsqrt(jnp.mean(gated * gated, axis=-1, keepdims=True) + EPSILON)
    normed = (gated * scale * gain[...]).astype(BF16)
    rows = outs[0].shape[0]
    for r, out in enumerate(outs):
        out[...] = normed[r * rows : (r + 1) * rows, :]


def output_body(where, *refs, count):
    pieces, (weight, own, oth, gate, out) = refs[: 2 * count], refs[2 * count : 2 * count + 5]
    left, right, rest, done, acc, sems = refs[2 * count + 5 :]
    half, n = pieces[0].shape
    n_out = out.shape[1]
    column = pl.multiple_of(where[1] * n_out, n_out)
    copies = []

    def start(source, target):
        copies.append(pltpu.make_async_copy(source, target, sems.at[len(copies)]))
        copies[-1].start()

    for b in range(count):
        at = pl.multiple_of(where[2 + b] * n, n)
        start(weight.at[pl.ds(at, n), :], right.at[b * n : (b + 1) * n, :])
        for p in range(2):
            start(
                pieces[2 * b + p],
                left.at[p * half : (p + 1) * half, b * n : (b + 1) * n],
            )
    start(own.at[:, pl.ds(column, n_out)], rest.at[0])
    start(oth.at[:, pl.ds(column, n_out)], rest.at[1])
    groups = count // 2
    for g in range(groups - 1):
        for copy in copies[6 * g : 6 * g + 6]:
            copy.wait()
        cut = slice(2 * g * n, 2 * (g + 1) * n)
        term = jnp.dot(left[:, cut], right[cut, :], preferred_element_type=F32)
        if g:
            acc[...] += term
        else:
            acc[...] = term
    for copy in copies[6 * (groups - 1) :]:
        copy.wait()
    cut = slice(2 * (groups - 1) * n, 2 * groups * n)
    writes = []
    for p in range(2):
        rows = slice(p * half, (p + 1) * half)
        total = acc[rows, :] + jnp.dot(left[rows, cut], right[cut, :], preferred_element_type=F32)
        mine = jnp.where(where[0] == p, 1.0, 0.0)
        base = rest[0].astype(F32) * mine + rest[1].astype(F32) * (1.0 - mine)
        done[rows, :] = (base + gate[...] * total).astype(BF16)
        writes.append(pltpu.make_async_copy(done.at[rows, :], out.at[rows, :], sems.at[p]))
        writes[-1].start()
    for write in writes:
        write.wait()


def whole(shape):
    return pl.BlockSpec(shape, lambda *_: (0,) * len(shape))


def shaped(shape, dtype):
    return pltpu.HBM(shape, dtype)


def placed(*arrays):
    return [pltpu.with_memory_space_constraint(a, pltpu.HBM) for a in arrays]


def in_vmem(*arrays):
    return [pltpu.with_memory_space_constraint(a, pltpu.VMEM) for a in arrays]


def on_device(
    latent, context, condition, context_condition, shift_weight, scale_weight, gate_weight,
    norm_gain, out_gate_weight, signal_weight, writer_weight, reader_matrix, step_weight,
    signal_taps, writer_taps, reader_taps, step_bias, decay_log, decay_extra, group_gain,
    output_weight,
):
    sp, tp, dp = lax.axis_index("sp"), lax.axis_index("tp"), lax.axis_index("dp")
    n_sp, n_tp, n_dp = lax.axis_size("sp"), lax.axis_size("tp"), lax.axis_size("dp")
    half, d_model = latent.shape
    length = half * n_dp
    ctx_len = context.shape[0]
    heads = step_bias.shape[1]
    n_sig = signal_weight.shape[1]
    n_gate = out_gate_weight.shape[1]
    n_state = writer_weight.shape[1]
    n_out = output_weight.shape[1]

    cols_here = shift_weight.shape[1]
    small = lambda n: pltpu.CompilerParams(vmem_limit_bytes=n * MIB)
    parts = pl.pallas_call(
        condense_body,
        out_shape=shaped((n_sp, 5 * cols_here // LANES, LANES), BF16),
        grid_spec=pltpu.PrefetchScalarGridSpec(
            num_scalar_prefetch=1,
            grid=(1,),
            in_specs=[whole((d_model // LANES, LANES))] * 2 + [whole(shift_weight.shape)] * 3,
            out_specs=whole((n_sp, 5 * cols_here // LANES, LANES)),
            scratch_shapes=[
                pltpu.VMEM((2 * d_model // LANES, LANES), F32),
                pltpu.VMEM((8 * cols_here // LANES, LANES), F32),
            ],
        ),
        compiler_params=small(8),
        name="condense",
    )(
        sp.astype(jnp.int32)[None],
        *placed(condition.reshape(-1, LANES), context_condition.reshape(-1, LANES)),
        *placed(shift_weight, scale_weight, gate_weight),
    )
    latent, context, sent = lax.optimization_barrier((latent, context, parts))
    sums = lax.all_to_all(sent, "sp", split_axis=0, concat_axis=0, tiled=True)
    vectors, gate_vec = pl.pallas_call(
        fold_body,
        out_shape=(
            shaped((n_tp * n_dp, 4 * cols_here // LANES, LANES), F32),
            shaped((1, cols_here), F32),
        ),
        compiler_params=pltpu.CompilerParams(vmem_limit_bytes=8 * MIB),
        name="fold",
    )(sums)
    vectors = lax.all_to_all(vectors, ("tp", "dp"), split_axis=0, concat_axis=0, tiled=True)

    oth = shifted(latent, "dp", 1)
    edge = jnp.where(
        dp == 1,
        jnp.concatenate([latent[-1:], context[-1:]]),
        jnp.concatenate([latent[:1], context[:1]]),
    )
    pairs = {0: [], 1: []}
    for s in range(n_sp):
        for flip in pairs:
            if s + 1 < n_sp:
                pairs[flip].append((2 * s + 1, 2 * (s + 1) + 1 - flip))
            if s:
                pairs[flip].append((2 * s, 2 * (s - 1) + flip))
    same = lax.ppermute(edge, ("sp", "dp"), pairs[0])
    crossed = lax.ppermute(edge, ("sp", "dp"), pairs[1])

    flags = jnp.stack([dp, sp == 0, sp == n_sp - 1]).astype(jnp.int32)
    n_all = n_gate + n_sig + 2 * n_state
    n_rows = length + ctx_len + 2 * EDGES
    part = n_sig // n_sp
    tail = KINDS * PIECES
    conv_w = n_sig + 2 * n_state
    k_tile = CHUNKS * cols_here
    tile = lambda rows: pl.BlockSpec((rows, k_tile), lambda k, *_: (0, k))
    down = lambda cols: pl.BlockSpec((k_tile, cols), lambda k, *_: (k, 0))
    outs = (
        shaped((length, n_gate), BF16),
        shaped((length, n_sig), BF16),
        shaped((length, n_state), BF16),
        shaped((length, n_state), BF16),
        shaped((4 * heads, length), F32),
        shaped((length, LANES), F32),
        shaped((n_sp, KINDS * part + tail, n_state), BF16),
    )
    gate_in, signal, writer, reader, rows, cols, payload = pl.pallas_call(
        functools.partial(project_body, heads=heads),
        out_shape=outs,
        grid_spec=pltpu.PrefetchScalarGridSpec(
            num_scalar_prefetch=1,
            grid=(d_model // k_tile,),
            in_specs=[
                tile(half), tile(half), tile(ctx_len), tile(2), tile(2),
                tile(1),
                pl.BlockSpec((CHUNKS, 4 * cols_here // LANES, LANES), lambda k, *_: (k, 0, 0)),
                down(n_gate), down(n_sig), down(n_state), down(n_state),
                pl.BlockSpec((2, heads, k_tile), lambda k, *_: (0, 0, k)),
                whole(signal_taps.shape), whole(writer_taps.shape), whole(reader_taps.shape),
                whole(step_bias.shape), whole(decay_log.shape), whole(decay_extra.shape),
            ],
            out_specs=[whole(o.shape) for o in outs],
            scratch_shapes=[
                pltpu.VMEM((n_rows, n_all), F32),
                pltpu.VMEM((n_rows, 2 * heads), F32),
                pltpu.VMEM((n_rows, LANES), F32),
                pltpu.VMEM((length + 16, conv_w), F32),
                pltpu.VMEM((ctx_len + 16, conv_w), F32),
                pltpu.VMEM((length + LANES, LANES), F32),
                pltpu.VMEM((2 * heads, cols_here), F32),
            ]
            + [pltpu.VMEM((n_rows, cols_here), BF16)] * CHUNKS,
        ),
        compiler_params=pltpu.CompilerParams(
            dimension_semantics=("arbitrary",), vmem_limit_bytes=28 * MIB
        ),
        cost_estimate=pl.CostEstimate(
            flops=2 * n_rows * d_model * n_all, transcendentals=0,
            bytes_accessed=2 * d_model * (n_rows + n_all),
        ),
        name="project",
    )(
        flags, *placed(latent), oth, *placed(context), same, crossed, *placed(norm_gain.reshape(1, -1)), vectors,
        *placed(out_gate_weight, signal_weight, writer_weight, reader_matrix),
        *placed(jnp.swapaxes(step_weight, 1, 2)), *placed(signal_taps, writer_taps, reader_taps),
        *placed(step_bias, decay_log, decay_extra),
    )

    got = lax.all_to_all(payload, "sp", split_axis=0, concat_axis=0, tiled=True)
    row_block = lambda cols_: pl.BlockSpec((I_TILE, cols_), lambda i: (i, 0))
    inside = pl.pallas_call(
        functools.partial(inside_body, heads=heads),
        out_shape=shaped((length, n_sig), F32),
        grid=(length // I_TILE,),
        in_specs=[
            row_block(n_state), whole((length, n_state)), whole((length, n_sig)),
            whole((4 * heads, length)), row_block(LANES),
        ],
        out_specs=row_block(n_sig),
        compiler_params=pltpu.CompilerParams(vmem_limit_bytes=16 * MIB),
        cost_estimate=pl.CostEstimate(
            flops=2 * length * length * (n_state + 4 * n_sig),
            transcendentals=heads * length * length,
            bytes_accessed=4 * length * n_sig,
        ),
        name="inside",
    )(*placed(reader, writer, signal, rows, cols))
    got, inside = lax.optimization_barrier((got, inside))
    starts = pl.pallas_call(
        functools.partial(chain_body, part=part),
        out_shape=shaped((n_sp, 2 * part, n_state), BF16),
        compiler_params=pltpu.CompilerParams(vmem_limit_bytes=4 * MIB),
        name="chain",
    )(got)
    starts = lax.all_to_all(starts, "sp", split_axis=0, concat_axis=0, tiled=True)
    normed = pl.pallas_call(
        functools.partial(finish_body, heads=heads),
        out_shape=[shaped((half, n_sig), BF16)] * n_dp,
        compiler_params=small(12),
        name="finish",
    )(starts, *placed(reader, cols, inside, gate_in), group_gain.reshape(1, -1))
    normed = placed(*normed)
    moved = {0: normed}
    for by in {1, n_tp - 1}:
        moved[by] = [shifted(piece, "tp", by) for piece in normed]
    for by in range(2, n_tp - 1):
        if n_tp == 4:
            moved[by] = [shifted(moved[1][0], "tp", 1), shifted(moved[3][1], "tp", 3)]
        else:
            moved[by] = [shifted(piece, "tp", by) for piece in normed]
    *held, _ = lax.optimization_barrier((*normed, moved[1][0]))
    pieces, places = [], []
    for by in (0, *(k for k in moved if k in (1, n_tp - 1)), *range(2, n_tp - 1)):
        place = (tp + n_tp - by) % n_tp * n_dp
        for blocks in (moved[by], [shifted(b, "dp", 1) for b in (moved[by] if by else held)]):
            pieces.extend(blocks)
        places += [place + dp, place + 1 - dp]
    at = tp * n_dp + dp
    where = jnp.stack([dp, at, *places]).astype(jnp.int32)
    count = len(places)
    anywhere = pl.BlockSpec(memory_space=pl.ANY)
    return pl.pallas_call(
        functools.partial(output_body, count=count),
        out_shape=shaped((length, n_out), BF16),
        grid_spec=pltpu.PrefetchScalarGridSpec(
            num_scalar_prefetch=1,
            grid=(1,),
            in_specs=[anywhere] * (2 * count + 3) + [whole((1, n_out))],
            out_specs=anywhere,
            scratch_shapes=[
                pltpu.VMEM((length, n_sig * count), BF16),
                pltpu.VMEM((n_sig * count, n_out), BF16),
                pltpu.VMEM((2, half, n_out), BF16),
                pltpu.VMEM((length, n_out), BF16),
                pltpu.VMEM((length, n_out), F32),
                pltpu.SemaphoreType.DMA((3 * count + 2,)),
            ],
        ),
        compiler_params=small(24),
        name="output",
    )(where, *placed(*pieces), *placed(output_weight, latent), oth, gate_vec)


def solution(mesh):
    tensor = ("tp", "dp")
    in_specs = (
        P(("grp", "sp", "dp"), None), P(("grp", "sp"), None), P("grp"), P(),
        P("sp", tensor), P("sp", tensor), P("sp", tensor), P(),
        P(None, tensor), P(None, tensor), P(None, tensor), P(None, tensor),
        P(None, None, tensor), P(None, tensor), P(None, tensor), P(None, tensor),
        P(None, tensor), P(None, tensor), P(None, tensor, ("grp", "sp")), P(tensor),
        P(None, tensor),
    )
    return jax.shard_map(
        on_device, mesh=mesh, in_specs=in_specs, out_specs=P(("grp", "sp"), tensor),
        check_vma=False,
    )
```
